32 devices in a mesh: sp: 8 (over z, x), tp: 4 (over y, core).
Axes of the slice: x: 2, y: 2, z: 4, core: 2. Of those that a mesh axis runs over, the one named last changes fastest.
Arguments:
- residual_in: bfloat16 [2048, 2048], P(('sp', 'tp')), may hold values from -0.119628906 to 0.119628906
- queries: bfloat16 [2048, 2048], P('sp', 'tp'), may hold values from -6 to 6
- keys_raw: bfloat16 [2048, 512], P('sp', 'tp'), may hold values from -6 to 6
- values_raw: bfloat16 [2048, 512], P('sp', 'tp'), may hold values from -6 to 6
- query_gain: float32 [128], replicated, may hold values from 0.28 to 7
- key_gain: float32 [128], replicated, may hold values from 0.28 to 7
- out_weight: bfloat16 [2048, 2048], P('tp'), may hold values from -0.125 to 0.125
- norm_gain: float32 [2048], replicated, may hold values from 0.1 to 1.9
- gate_weight: bfloat16 [2048, 5632], P('sp', 'tp'), may hold values from -0.125 to 0.125
- up_weight: bfloat16 [2048, 5632], P('sp', 'tp'), may hold values from -0.125 to 0.125
- down_weight: bfloat16 [5632, 2048], P('tp', 'sp'), may hold values from -0.078125 to 0.078125
Outputs:
- residual_out: bfloat16 [2048, 2048], P(('sp', 'tp'))
The draws below stay inside these ranges and needn't reach their ends.
All inputs are finite; a program needn't handle non-finite values.
Results may differ from the reference program's by a relative error of at most 0.024.
The reference program's roundings to bfloat16 on the way count: a program that leaves them out, or rounds other values in their place, can miss the bound.
Values may be sent and summed in bfloat16 or wider, within the bound.
A program may use at most 128 MiB of HBM per device.

```python
import math
import jax
import jax.numpy as jnp
from jax import lax

D = 2048
H = 16
KVH = 4
HD = 128
FF = 5632
GRID_W = 64
TOKENS = 2048
N_TP = 4


def paired_rows(key):
    keys_part = jnp.clip(jax.random.normal(jax.random.fold_in(key, 11), (TOKENS, KVH * HD), jnp.float32), -6.0, 6.0)
    query_part = jnp.clip(jax.random.normal(jax.random.fold_in(key, 12), (TOKENS, H * HD), jnp.float32), -6.0, 6.0)
    return (query_part, keys_part)


def draw_queries(key, part):
    return paired_rows(key)[0].astype(jnp.bfloat16)


def draw_keys_raw(key, part):
    return paired_rows(key)[1].astype(jnp.bfloat16)


def gain_draw(key):
    return 1.0 + 0.18 * jnp.clip(jax.random.normal(key, (HD,), jnp.float32), -4.0, 4.0)


def draw_query_gain(key, part):
    return gain_draw(jax.random.fold_in(key, 21))


def draw_key_gain(key, part):
    return gain_draw(jax.random.fold_in(key, 22))


def levels(own_key, dims, pieces, smallest, high):
    def one(dim, shards_of):
        draws = jax.random.uniform(jax.random.fold_in(jax.random.fold_in(own_key, 6), dim), (shards_of,), jnp.float32, smallest / len(pieces), high / len(pieces))
        return jnp.repeat(jnp.exp(draws), dims[dim] // shards_of).reshape((-1,) + (1,) * (len(dims) - dim - 1))

    level = one(*pieces[0])
    for cut in pieces[1:]:
        level = level * one(*cut)
    return level


def gaussian(key, extent, spread, limit, pieces=(), held_as=jnp.bfloat16):
    result = jax.random.normal(key, extent, jnp.float32) * spread
    if len(pieces) > 0:
        result = levels(key, extent, pieces, -0.22, 0.18) * result
    return jnp.clip(result, min=-limit, max=limit).astype(held_as)


def setup_inputs(seed: int = 0) -> dict:
    key_of = jax.random.split(jax.random.key(seed), 12)
    residual_in = gaussian(key_of[0], (TOKENS, D), 0.02, 0.119628906, ((0, 32),))
    queries = draw_queries(jax.random.fold_in(key_of[11], 71), 0)
    keys_raw = draw_keys_raw(jax.random.fold_in(key_of[11], 71), 0)
    values_raw = gaussian(key_of[3], (TOKENS, KVH * HD), 1.0, 6.0, ((0, 8), (1, 4)))
    query_gain = draw_query_gain(jax.random.fold_in(key_of[11], 71), 0)
    key_gain = draw_key_gain(jax.random.fold_in(key_of[11], 71), 0)
    out_weight = gaussian(key_of[6], (H * HD, D), (H * HD) ** -0.5, 0.125, ((0, 4),))
    norm_gain = jnp.clip(1.0 + 0.18 * jax.random.normal(key_of[7], (D,), jnp.float32), 0.1, 1.9)
    gate_weight = gaussian(key_of[8], (D, FF), D ** -0.5, 0.125, ((0, 8), (1, 4)))
    up_weight = gaussian(key_of[9], (D, FF), D ** -0.5, 0.125, ((0, 8), (1, 4)))
    down_weight = gaussian(key_of[10], (FF, D), FF ** -0.5, 0.078125, ((0, 4), (1, 8)))
    return {"residual_in": residual_in, "queries": queries, "keys_raw": keys_raw, "values_raw": values_raw, "query_gain": query_gain, "key_gain": key_gain, "out_weight": out_weight, "norm_gain": norm_gain, "gate_weight": gate_weight, "up_weight": up_weight, "down_weight": down_weight}


EPS = 1e-06
THETA = 10000.0

def turn_half(part, angles):
    quarter = part.shape[-1] // 2
    cosine = jnp.cos(angles)[:, None, :]
    sine = jnp.sin(angles)[:, None, :]
    first = part[..., :quarter]
    second = part[..., quarter:]
    return part * cosine + jnp.concatenate([-second, first], axis=-1) * sine

def prepare_heads(raw, gain, positions, heads):
    count = raw.shape[0]
    head_dim = gain.shape[0]
    half = head_dim // 2
    vec = raw.astype(jnp.float32).reshape(count, heads, head_dim)
    vec = vec * lax.rsqrt(lax.optimization_barrier(jnp.mean(vec * vec, axis=-1, keepdims=True)) + EPS) * gain
    freqs = THETA ** (-jnp.arange(0, half, 2, dtype=jnp.float32) / half)
    row_ang = (positions // GRID_W).astype(jnp.float32)[:, None] * freqs
    col_ang = (positions % GRID_W).astype(jnp.float32)[:, None] * freqs
    row_ang = jnp.concatenate([row_ang, row_ang], axis=-1)
    col_ang = jnp.concatenate([col_ang, col_ang], axis=-1)
    turned = jnp.concatenate([turn_half(vec[..., :half], row_ang), turn_half(vec[..., half:], col_ang)], axis=-1)
    return turned.astype(jnp.bfloat16)

def reference(residual_in, queries, keys_raw, values_raw, query_gain, key_gain, out_weight, norm_gain, gate_weight, up_weight, down_weight):
    positions = jnp.arange(TOKENS, dtype=jnp.int32)
    group = H // KVH
    q_rot = prepare_heads(queries, query_gain, positions, H)
    k_rot = prepare_heads(keys_raw, key_gain, positions, KVH).astype(jnp.float32)
    vals = values_raw.reshape(TOKENS, KVH, HD).astype(jnp.float32)
    block = math.gcd(TOKENS, 256)
    q_blocks = q_rot.reshape(TOKENS // block, block, KVH, group, HD)

    def attend(q_blk):
        scores = jnp.einsum('qkgd,skd->qkgs', q_blk.astype(jnp.float32), k_rot) * HD ** (-0.5)
        top = lax.optimization_barrier(jnp.max(scores, axis=-1, keepdims=True))
        expo = jnp.exp(scores - top)
        total = lax.optimization_barrier(jnp.sum(expo, axis=-1))
        rounded = lax.optimization_barrier(expo.astype(jnp.bfloat16)).astype(jnp.float32)
        summed = jnp.einsum('qkgs,skd->qkgd', rounded, vals)
        return (summed / total[..., None]).astype(jnp.bfloat16)
    attended = lax.map(attend, q_blocks).reshape(TOKENS, H * HD)
    head_cols = H * HD // N_TP
    projected = jnp.zeros((TOKENS, D), jnp.float32)
    for grp in range(N_TP):
        term = jnp.dot(attended[:, grp * head_cols:(grp + 1) * head_cols], out_weight[grp * head_cols:(grp + 1) * head_cols], preferred_element_type=jnp.float32)
        projected = projected + lax.optimization_barrier(term.astype(jnp.bfloat16)).astype(jnp.float32)
    mixed = (residual_in.astype(jnp.float32) + projected).astype(jnp.bfloat16)
    mixed_f = mixed.astype(jnp.float32)
    normed = (mixed_f * lax.rsqrt(lax.optimization_barrier(jnp.mean(mixed_f * mixed_f, axis=-1, keepdims=True)) + EPS) * norm_gain).astype(jnp.bfloat16)
    gate = jnp.dot(normed, gate_weight, preferred_element_type=jnp.float32)
    up_val = jnp.dot(normed, up_weight, preferred_element_type=jnp.float32)
    hidden = (jax.nn.silu(gate) * up_val).astype(jnp.bfloat16)
    unit_rows = FF // N_TP
    fed = jnp.zeros((TOKENS, D), jnp.float32)
    for grp in range(N_TP):
        term = jnp.dot(hidden[:, grp * unit_rows:(grp + 1) * unit_rows], down_weight[grp * unit_rows:(grp + 1) * unit_rows], preferred_element_type=jnp.float32)
        fed = fed + lax.optimization_barrier(term.astype(jnp.bfloat16)).astype(jnp.float32)
    return (mixed_f + 0.5 * fed).astype(jnp.bfloat16)
```

```python
import jax
import jax.numpy as jnp
from jax import lax
from jax.experimental import pallas as pl
from jax.experimental.pallas import tpu as pltpu
import functools
from jax.sharding import PartitionSpec as P

GRID_W = 64


EPS = 1e-06
THETA = 10000.0


def turn_half(part, angles):
    quarter = part.shape[-1] // 2
    cosine = jnp.cos(angles)[:, None, :]
    sine = jnp.sin(angles)[:, None, :]
    first = part[..., :quarter]
    second = part[..., quarter:]
    return part * cosine + jnp.concatenate([-second, first], axis=-1) * sine


def prepare_heads(raw, gain, positions, heads):
    count = raw.shape[0]
    head_dim = gain.shape[0]
    half = head_dim // 2
    vec = raw.astype(jnp.float32).reshape(count, heads, head_dim)
    vec = vec * lax.rsqrt(jnp.mean(vec * vec, axis=-1, keepdims=True) + EPS) * gain
    freqs = THETA ** (-jnp.arange(0, half, 2, dtype=jnp.float32) / half)
    row_ang = (positions // GRID_W).astype(jnp.float32)[:, None] * freqs
    col_ang = (positions % GRID_W).astype(jnp.float32)[:, None] * freqs
    row_ang = jnp.concatenate([row_ang, row_ang], axis=-1)
    col_ang = jnp.concatenate([col_ang, col_ang], axis=-1)
    turned = jnp.concatenate(
        [turn_half(vec[..., :half], row_ang), turn_half(vec[..., half:], col_ang)], axis=-1
    )
    return turned.astype(jnp.bfloat16)


def plain_device(
    residual_in,
    queries,
    keys_raw,
    values_raw,
    query_gain,
    key_gain,
    out_weight,
    norm_gain,
    gate_weight,
    up_weight,
    down_weight,
):
    tok = queries.shape[0]
    head_dim = query_gain.shape[0]
    local_heads = queries.shape[1] // head_dim
    local_kv = keys_raw.shape[1] // head_dim
    group = local_heads // local_kv
    gate_full, up_full = (
        lax.all_gather(gate_weight, "sp", axis=0, tiled=True),
        lax.all_gather(up_weight, "sp", axis=0, tiled=True),
    )
    down_full = lax.all_gather(down_weight, "sp", axis=1, tiled=True)
    positions = lax.axis_index("sp") * tok + jnp.arange(tok, dtype=jnp.int32)
    q_rot = prepare_heads(queries, query_gain, positions, local_heads).reshape(
        tok, local_kv, group, head_dim
    )
    k_rot = prepare_heads(keys_raw, key_gain, positions, local_kv)
    vals = values_raw.reshape(tok, local_kv, head_dim)
    start_state = (
        jnp.full((tok, local_kv, group), -jnp.inf, jnp.float32),
        jnp.zeros((tok, local_kv, group), jnp.float32),
        jnp.zeros((tok, local_kv, group, head_dim), jnp.float32),
    )
    carry = start_state
    k_piece = lax.all_gather(k_rot, "sp", axis=0, tiled=True)
    v_piece = lax.all_gather(vals, "sp", axis=0, tiled=True)
    length = k_piece.shape[0]
    shards = length // tok
    per_step = max(1, 2048 // tok)
    factor = max((d for d in range(1, shards + 1) if shards % d == 0 and d <= per_step))
    span = factor * tok
    k_blocks = k_piece.reshape(length // span, span, local_kv, head_dim)
    v_blocks = v_piece.reshape(length // span, span, local_kv, head_dim)

    def step(state, blocks):
        top, total, summed = state
        k_blk, v_blk = blocks
        scores = jnp.einsum(
            "qkgd,skd->qkgs", q_rot, k_blk, preferred_element_type=jnp.float32
        ) * head_dim ** (-0.5)
        new_top = jnp.maximum(top, jnp.max(scores, axis=-1))
        shrink = jnp.exp(top - new_top)
        expo = jnp.exp(scores - new_top[..., None])
        total = total * shrink + jnp.sum(expo, axis=-1)
        summed = summed * shrink[..., None] + jnp.einsum(
            "qkgs,skd->qkgd", expo.astype(jnp.bfloat16), v_blk, preferred_element_type=jnp.float32
        )
        return ((new_top, total, summed), None)

    carry, _ = lax.scan(step, carry, (k_blocks, v_blocks))
    top, total, summed = carry
    attended = (summed / total[..., None]).astype(jnp.bfloat16).reshape(tok, local_heads * head_dim)
    projected = lax.psum_scatter(
        jnp.dot(attended, out_weight, preferred_element_type=jnp.float32).astype(jnp.bfloat16),
        "tp",
        scatter_dimension=0,
        tiled=True,
    ).astype(jnp.float32)
    mixed = (residual_in.astype(jnp.float32) + projected).astype(jnp.bfloat16)
    mixed_f = mixed.astype(jnp.float32)
    normed = (
        mixed_f * lax.rsqrt(jnp.mean(mixed_f * mixed_f, axis=-1, keepdims=True) + EPS) * norm_gain
    ).astype(jnp.bfloat16)
    whole_rows = lax.all_gather(normed, "tp", axis=0, tiled=True)
    gate = jnp.dot(whole_rows, gate_full, preferred_element_type=jnp.float32)
    up_val = jnp.dot(whole_rows, up_full, preferred_element_type=jnp.float32)
    hidden = (jax.nn.silu(gate) * up_val).astype(jnp.bfloat16)
    terms = jnp.dot(hidden, down_full, preferred_element_type=jnp.float32)
    fed = lax.psum_scatter(
        terms.astype(jnp.bfloat16), "tp", scatter_dimension=0, tiled=True
    ).astype(jnp.float32)
    return (mixed_f + 0.5 * fed).astype(jnp.bfloat16)


NX = 2
NC = 2
LANES = 128


def ring_kernel(
    nz,
    res_ref, q_ref, k_ref, v_ref, cos_ref, sin_ref, qg_ref, kg_ref, ow_ref, ng_ref, g_ref, u_ref, d_ref,
    out_ref,
    k_own, k_all, v_all, g_all, u_all, d_all, q_s, att_s, proj, proj_in, normed_all,
    part, core_in, y_out, y_in, z_out, z_in, mixed_s,
    kz_s, kz_r, kx_s, kx_r, wz_s, wz_r, wx_s, wx_r, pj_s, pj_r,
    nz_s, nz_r, ny_s, ny_r, nc_s, nc_r, nf_s, nf_r,
    c_s, c_r, y_s, y_r, z_s, z_r,
):
    f32, bf16 = jnp.float32, jnp.bfloat16
    sp, tp = lax.axis_index("sp"), lax.axis_index("tp")
    z, x = sp // NX, sp % NX
    y, c = tp // NC, tp % NC
    ntp = 2 * NC
    tok = q_ref.shape[0]
    hd = k_ref.shape[1]
    heads = q_ref.shape[1] // hd
    rows = res_ref.shape[0]
    wide = res_ref.shape[1]
    drows = g_ref.shape[0]
    unit = g_all.shape[1]

    def at_z(zz):
        return (zz * NX + x, tp)

    x_peer = (z * NX + (1 - x), tp)
    y_peer = (sp, (1 - y) * NC + c)
    c_peer = (sp, y * NC + (1 - c))

    def up(d):
        return lax.rem(z + d, nz)

    def down(d):
        return lax.rem(z + nz - d, nz)

    def rc(src, dst, ss, rs, dev):
        return pltpu.make_async_remote_copy(
            src_ref=src, dst_ref=dst, send_sem=ss, recv_sem=rs, device_id=dev,
            device_id_type=pl.DeviceIdType.MESH,
        )

    barrier = pltpu.get_barrier_semaphore()
    peers = [at_z(up(d)) for d in range(1, nz)] + [x_peer]
    peers += [(sp, lax.rem(tp + e, ntp)) for e in range(1, ntp)]
    for dev in peers:
        pl.semaphore_signal(barrier, inc=1, device_id=dev, device_id_type=pl.DeviceIdType.MESH)
    pl.semaphore_wait(barrier, len(peers))

    lane = lax.broadcasted_iota(jnp.int32, (tok, hd), 1)
    low = (lane % (hd // 2)) < (hd // 4)
    cosine, sine = cos_ref[...], sin_ref[...]

    def prepare(raw, gain):
        vec = raw.astype(f32)
        vec = vec * lax.rsqrt(jnp.mean(vec * vec, axis=-1, keepdims=True) + EPS) * gain
        swapped = jnp.where(low, pltpu.roll(vec, hd - hd // 4, 1), pltpu.roll(vec, hd // 4, 1))
        return (vec * cosine + swapped * sine).astype(bf16)

    def tok_rows(s):
        return pl.ds(pl.multiple_of(s * tok, tok), tok)

    def w_rows(s):
        return pl.ds(pl.multiple_of(s * drows, drows), drows)

    def w_cols(zz):
        return pl.ds(pl.multiple_of(zz * unit, unit), unit)

    k_new = prepare(k_ref[...], kg_ref[...])
    k_own[...] = k_new
    mine = tok_rows(sp)
    k_all[mine, :] = k_new
    v_all[mine, :] = v_ref[...]

    kz = []
    for d in range(1, nz):
        kz.append((
            rc(k_own, k_all.at[mine, :], kz_s.at[0, d], kz_r.at[0, d], at_z(up(d))),
            rc(v_ref, v_all.at[mine, :], kz_s.at[1, d], kz_r.at[1, d], at_z(up(d))),
        ))
        for op in kz[-1]:
            op.start()
    kx = [(
        rc(k_own, k_all.at[mine, :], kx_s.at[0, 0], kx_r.at[0, 0], x_peer),
        rc(v_ref, v_all.at[mine, :], kx_s.at[1, 0], kx_r.at[1, 0], x_peer),
    )]
    for op in kx[0]:
        op.start()

    def pieces(zz, s_sem, r_sem, i, dev):
        return (
            rc(g_ref.at[:, w_cols(zz)], g_all.at[w_rows(sp), :], s_sem.at[0, i], r_sem.at[0, i], dev),
            rc(u_ref.at[:, w_cols(zz)], u_all.at[w_rows(sp), :], s_sem.at[1, i], r_sem.at[1, i], dev),
            rc(d_ref.at[w_cols(zz), :], d_all.at[sp], s_sem.at[2, i], r_sem.at[2, i], dev),
        )

    wz = []
    for d in range(1, nz):
        wz.append(pieces(up(d), wz_s, wz_r, d, at_z(up(d))))
        for op in wz[-1]:
            op.start()

    for h in range(heads):
        q_s[h] = prepare(q_ref[:, h * hd:(h + 1) * hd], qg_ref[...])
    g_all[w_rows(sp), :] = g_ref[:, w_cols(z)]
    u_all[w_rows(sp), :] = u_ref[:, w_cols(z)]
    d_all[sp] = d_ref[w_cols(z), :]

    for d in range(1, nz):
        for op in kz[d - 1]:
            op.wait_recv()
        theirs = tok_rows(down(d) * NX + x)
        kx.append((
            rc(k_all.at[theirs, :], k_all.at[theirs, :], kx_s.at[0, d], kx_r.at[0, d], x_peer),
            rc(v_all.at[theirs, :], v_all.at[theirs, :], kx_s.at[1, d], kx_r.at[1, d], x_peer),
        ))
        for op in kx[-1]:
            op.start()
    wx = [pieces(z, wx_s, wx_r, 0, x_peer)]
    for op in wx[0]:
        op.start()
    for pair in kx:
        for op in pair:
            op.wait_recv()

    scale = hd ** (-0.5)
    for h in range(heads):
        scores = lax.dot_general(
            q_s[h], k_all[...], (((1,), (1,)), ((), ())), preferred_element_type=f32
        )
        top = jnp.max(scores, axis=-1, keepdims=True)
        expo = jnp.exp((scores - top) * scale)
        total = jnp.sum(expo, axis=-1, keepdims=True)
        summed = jnp.dot(expo.astype(bf16), v_all[...], preferred_element_type=f32)
        att_s[:, h * hd:(h + 1) * hd] = (summed / total).astype(bf16)

    step = wide // 4
    for i in range(4):
        cols = slice(i * step, (i + 1) * step)
        prod = jnp.dot(att_s[...], ow_ref[:, cols], preferred_element_type=f32)
        proj[:, :, cols] = prod.astype(bf16).reshape(ntp, rows, step)
    pj = []
    for e in range(1, ntp):
        to = lax.rem(tp + e, ntp)
        pj.append(rc(proj.at[to], proj_in.at[e - 1], pj_s.at[e], pj_r.at[e], (sp, to)))
        pj[-1].start()

    def forward_weights(d):
        for op in wz[d - 1]:
            op.wait_recv()
        s = down(d) * NX + x
        wx.append((
            rc(g_all.at[w_rows(s), :], g_all.at[w_rows(s), :], wx_s.at[0, d], wx_r.at[0, d], x_peer),
            rc(u_all.at[w_rows(s), :], u_all.at[w_rows(s), :], wx_s.at[1, d], wx_r.at[1, d], x_peer),
            rc(d_all.at[s], d_all.at[s], wx_s.at[2, d], wx_r.at[2, d], x_peer),
        ))
        for op in wx[-1]:
            op.start()

    for op in pj:
        op.wait_recv()
    projected = proj[tp].astype(f32)
    for e in range(1, ntp):
        projected = projected + proj_in[e - 1].astype(f32)
    mixed = (res_ref[...].astype(f32) + projected).astype(bf16)
    mixed_s[...] = mixed
    mixed_f = mixed.astype(f32)
    normed = (
        mixed_f * lax.rsqrt(jnp.mean(mixed_f * mixed_f, axis=-1, keepdims=True) + EPS) * ng_ref[...]
    ).astype(bf16)
    own = z * ntp + tp
    normed_all[own] = normed

    nz_ops, ny_ops, nc_ops, nf_ops = [], [], [], []

    def pass_on(d):
        b = down(d) * ntp + tp
        blk = normed_all.at[b]
        ny_ops.append(rc(blk, blk, ny_s.at[d], ny_r.at[d], y_peer))
        nc_ops.append(rc(blk, blk, nc_s.at[d], nc_r.at[d], c_peer))
        ny_ops[-1].start()
        nc_ops[-1].start()

    def pass_over(d):
        ny_ops[d].wait_recv()
        blk = normed_all.at[down(d) * ntp + (1 - y) * NC + c]
        nf_ops.append(rc(blk, blk, nf_s.at[d], nf_r.at[d], c_peer))
        nf_ops[-1].start()

    for d in range(1, nz):
        blk = normed_all.at[own]
        nz_ops.append(rc(blk, blk, nz_s.at[d], nz_r.at[d], at_z(up(d))))
        nz_ops[-1].start()
    pass_on(0)
    for d in range(1, nz):
        forward_weights(d)
    pass_over(0)
    for d in range(1, nz):
        nz_ops[d - 1].wait_recv()
        pass_on(d)
    for d in range(1, nz):
        pass_over(d)
    for ops in wx:
        for op in ops:
            op.wait_recv()
    for op in nc_ops + nf_ops:
        op.wait_recv()

    def core_ops(d, j):
        b = up(d) * ntp + j * NC + (1 - c)
        return rc(part.at[b], core_in.at[d, j], c_s.at[d, j], c_r.at[d, j], c_peer)

    cols_each = d_all.shape[2]

    def tile(i, carry):
        d = lax.rem(i + 1, nz)
        t = up(d)
        x_t = normed_all[pl.ds(t * ntp, ntp)].reshape(ntp * rows, wide)
        gate = jnp.dot(x_t, g_all[...], preferred_element_type=f32)
        up_val = jnp.dot(x_t, u_all[...], preferred_element_type=f32)
        hidden = (gate / (1.0 + jnp.exp(-gate)) * up_val).astype(bf16)
        for s in range(d_all.shape[0]):
            r = jnp.dot(hidden, d_all[s], preferred_element_type=f32).astype(bf16)
            part[pl.ds(t * ntp, ntp), :, s * cols_each:(s + 1) * cols_each] = r.reshape(ntp, rows, cols_each)
        for j in range(2):
            core_ops(d, j).start()
        return carry

    lax.fori_loop(0, nz, tile, 0)

    y_ops = {}
    order = list(range(1, nz)) + [0]
    for d in order:
        for j in range(2):
            core_ops(d, j).wait_recv()
        b = up(d) * ntp + (1 - y) * NC + c
        y_out[d] = (part[b].astype(f32) + core_in[d, 1 - y].astype(f32)).astype(bf16)
        y_ops[d] = rc(y_out.at[d], y_in.at[d], y_s.at[d], y_r.at[d], y_peer)
        y_ops[d].start()

    def summed_tile(d):
        b = up(d) * ntp + tp
        return part[b].astype(f32) + core_in[d, y].astype(f32) + y_in[d].astype(f32)

    z_ops = []
    for d in range(1, nz):
        y_ops[d].wait_recv()
        z_out[d - 1] = summed_tile(d).astype(bf16)
        z_ops.append(rc(z_out.at[d - 1], z_in.at[d - 1], z_s.at[d], z_r.at[d], at_z(up(d))))
        z_ops[-1].start()
    y_ops[0].wait_recv()
    fed = summed_tile(0)
    for d in range(1, nz):
        z_ops[d - 1].wait_recv()
        fed = fed + z_in[d - 1].astype(f32)
    out_ref[...] = (mixed_s[...].astype(f32) + 0.5 * fed).astype(bf16)

    for ops in kz + kx + wz + wx:
        for op in ops:
            op.wait_send()
    for op in pj + nz_ops + ny_ops + nc_ops + nf_ops + z_ops + [y_ops[d] for d in order]:
        op.wait_send()
    for d in order:
        for j in range(2):
            core_ops(d, j).wait_send()


def ring_device(
    nsp,
    residual_in, queries, keys_raw, values_raw, query_gain, key_gain, out_weight, norm_gain,
    gate_weight, up_weight, down_weight,
):
    bf16 = jnp.bfloat16
    nz = nsp // NX
    tok = queries.shape[0]
    hd = query_gain.shape[0]
    heads = queries.shape[1] // hd
    rows, wide = residual_in.shape
    drows, units = gate_weight.shape
    ntp = tok // rows
    unit = -(-units // (nz * LANES)) * LANES
    extra = nz * unit - units
    gate_p = jnp.pad(gate_weight, ((0, 0), (0, extra)))
    up_p = jnp.pad(up_weight, ((0, 0), (0, extra)))
    down_p = jnp.pad(down_weight, ((0, extra), (0, 0)))
    half = hd // 2
    positions = lax.axis_index("sp") * tok + jnp.arange(tok, dtype=jnp.int32)
    freqs = THETA ** (-jnp.arange(0, half, 2, dtype=jnp.float32) / half)
    row_ang = (positions // GRID_W).astype(jnp.float32)[:, None] * freqs
    col_ang = (positions % GRID_W).astype(jnp.float32)[:, None] * freqs
    angles = jnp.concatenate([row_ang, row_ang, col_ang, col_ang], axis=-1)
    sign = jnp.where(jnp.arange(hd) % half < half // 2, -1.0, 1.0)
    cosine, sine = jnp.cos(angles), jnp.sin(angles) * sign
    dma = pltpu.SemaphoreType.DMA
    vm = pltpu.VMEM
    blk = (rows, wide)
    scratch = [
        vm((tok, hd), bf16), vm((nsp * tok, hd), bf16), vm((nsp * tok, hd), bf16),
        vm((nsp * drows, unit), bf16), vm((nsp * drows, unit), bf16), vm((nsp, unit, down_weight.shape[1]), bf16),
        vm((heads, tok, hd), bf16), vm((tok, heads * hd), bf16),
        vm((ntp,) + blk, bf16), vm((ntp - 1,) + blk, bf16), vm((nz * ntp,) + blk, bf16),
        vm((nz * ntp,) + blk, bf16), vm((nz, 2) + blk, bf16), vm((nz,) + blk, bf16), vm((nz,) + blk, bf16),
        vm((nz - 1,) + blk, bf16), vm((nz - 1,) + blk, bf16), vm(blk, bf16),
        dma((2, nz)), dma((2, nz)), dma((2, nz)), dma((2, nz)),
        dma((3, nz)), dma((3, nz)), dma((3, nz)), dma((3, nz)),
        dma((ntp,)), dma((ntp,)),
    ] + [dma((nz,)) for _ in range(8)] + [
        dma((nz, 2)), dma((nz, 2)), dma((nz,)), dma((nz,)), dma((nz,)), dma((nz,)),
    ]
    return pl.pallas_call(
        functools.partial(ring_kernel, nz),
        out_shape=jax.ShapeDtypeStruct(blk, bf16),
        in_specs=[pl.BlockSpec(memory_space=pltpu.VMEM)] * 13,
        out_specs=pl.BlockSpec(memory_space=pltpu.VMEM),
        scratch_shapes=scratch,
        compiler_params=pltpu.CompilerParams(
            collective_id=0, has_side_effects=True, vmem_limit_bytes=60 * 1024 * 1024
        ),
    )(
        residual_in, queries, keys_raw, values_raw, cosine, sine, query_gain[None], key_gain[None],
        out_weight, norm_gain[None], gate_p, up_p, down_p,
    )


def solution(mesh):
    nsp, ntp = mesh.shape["sp"], mesh.shape["tp"]

    def per_device(*arrays):
        residual_in, queries, keys_raw = arrays[:3]
        hd = arrays[4].shape[0]
        small = (
            nsp == 8 and ntp == 2 * NC and keys_raw.shape[1] == hd
            and queries.shape[0] == ntp * residual_in.shape[0]
            and arrays[8].shape[0] % LANES == 0 and queries.shape[0] <= 256
        )
        if small:
            return ring_device(nsp, *arrays)
        return plain_device(*arrays)

    placed = (
        P(("sp", "tp"), None),
        P("sp", "tp"),
        P("sp", "tp"),
        P("sp", "tp"),
        P(),
        P(),
        P("tp", None),
        P(),
        P("sp", "tp"),
        P("sp", "tp"),
        P("tp", "sp"),
    )
    return jax.shard_map(
        per_device, mesh=mesh, in_specs=placed, out_specs=P(("sp", "tp"), None), check_vma=False
    )
```

```python
import jax
import jax.numpy as jnp
from jax import lax
from jax.experimental import pallas as pl
from jax.experimental.pallas import tpu as pltpu
import functools
from jax.sharding import PartitionSpec as P

GRID_W = 64


EPS = 1e-06
THETA = 10000.0


def turn_half(part, angles):
    quarter = part.shape[-1] // 2
    cosine = jnp.cos(angles)[:, None, :]
    sine = jnp.sin(angles)[:, None, :]
    first = part[..., :quarter]
    second = part[..., quarter:]
    return part * cosine + jnp.concatenate([-second, first], axis=-1) * sine


def prepare_heads(raw, gain, positions, heads):
    count = raw.shape[0]
    head_dim = gain.shape[0]
    half = head_dim // 2
    vec = raw.astype(jnp.float32).reshape(count, heads, head_dim)
    vec = vec * lax.rsqrt(jnp.mean(vec * vec, axis=-1, keepdims=True) + EPS) * gain
    freqs = THETA ** (-jnp.arange(0, half, 2, dtype=jnp.float32) / half)
    row_ang = (positions // GRID_W).astype(jnp.float32)[:, None] * freqs
    col_ang = (positions % GRID_W).astype(jnp.float32)[:, None] * freqs
    row_ang = jnp.concatenate([row_ang, row_ang], axis=-1)
    col_ang = jnp.concatenate([col_ang, col_ang], axis=-1)
    turned = jnp.concatenate(
        [turn_half(vec[..., :half], row_ang), turn_half(vec[..., half:], col_ang)], axis=-1
    )
    return turned.astype(jnp.bfloat16)


def plain_device(
    residual_in,
    queries,
    keys_raw,
    values_raw,
    query_gain,
    key_gain,
    out_weight,
    norm_gain,
    gate_weight,
    up_weight,
    down_weight,
):
    tok = queries.shape[0]
    head_dim = query_gain.shape[0]
    local_heads = queries.shape[1] // head_dim
    local_kv = keys_raw.shape[1] // head_dim
    group = local_heads // local_kv
    gate_full, up_full = (
        lax.all_gather(gate_weight, "sp", axis=0, tiled=True),
        lax.all_gather(up_weight, "sp", axis=0, tiled=True),
    )
    down_full = lax.all_gather(down_weight, "sp", axis=1, tiled=True)
    positions = lax.axis_index("sp") * tok + jnp.arange(tok, dtype=jnp.int32)
    q_rot = prepare_heads(queries, query_gain, positions, local_heads).reshape(
        tok, local_kv, group, head_dim
    )
    k_rot = prepare_heads(keys_raw, key_gain, positions, local_kv)
    vals = values_raw.reshape(tok, local_kv, head_dim)
    start_state = (
        jnp.full((tok, local_kv, group), -jnp.inf, jnp.float32),
        jnp.zeros((tok, local_kv, group), jnp.float32),
        jnp.zeros((tok, local_kv, group, head_dim), jnp.float32),
    )
    carry = start_state
    k_piece = lax.all_gather(k_rot, "sp", axis=0, tiled=True)
    v_piece = lax.all_gather(vals, "sp", axis=0, tiled=True)
    length = k_piece.shape[0]
    shards = length // tok
    per_step = max(1, 2048 // tok)
    factor = max((d for d in range(1, shards + 1) if shards % d == 0 and d <= per_step))
    span = factor * tok
    k_blocks = k_piece.reshape(length // span, span, local_kv, head_dim)
    v_blocks = v_piece.reshape(length // span, span, local_kv, head_dim)

    def step(state, blocks):
        top, total, summed = state
        k_blk, v_blk = blocks
        scores = jnp.einsum(
            "qkgd,skd->qkgs", q_rot, k_blk, preferred_element_type=jnp.float32
        ) * head_dim ** (-0.5)
        new_top = jnp.maximum(top, jnp.max(scores, axis=-1))
        shrink = jnp.exp(top - new_top)
        expo = jnp.exp(scores - new_top[..., None])
        total = total * shrink + jnp.sum(expo, axis=-1)
        summed = summed * shrink[..., None] + jnp.einsum(
            "qkgs,skd->qkgd", expo.astype(jnp.bfloat16), v_blk, preferred_element_type=jnp.float32
        )
        return ((new_top, total, summed), None)

    carry, _ = lax.scan(step, carry, (k_blocks, v_blocks))
    top, total, summed = carry
    attended = (summed / total[..., None]).astype(jnp.bfloat16).reshape(tok, local_heads * head_dim)
    projected = lax.psum_scatter(
        jnp.dot(attended, out_weight, preferred_element_type=jnp.float32).astype(jnp.bfloat16),
        "tp",
        scatter_dimension=0,
        tiled=True,
    ).astype(jnp.float32)
    mixed = (residual_in.astype(jnp.float32) + projected).astype(jnp.bfloat16)
    mixed_f = mixed.astype(jnp.float32)
    normed = (
        mixed_f * lax.rsqrt(jnp.mean(mixed_f * mixed_f, axis=-1, keepdims=True) + EPS) * norm_gain
    ).astype(jnp.bfloat16)
    whole_rows = lax.all_gather(normed, "tp", axis=0, tiled=True)
    gate = jnp.dot(whole_rows, gate_full, preferred_element_type=jnp.float32)
    up_val = jnp.dot(whole_rows, up_full, preferred_element_type=jnp.float32)
    hidden = (jax.nn.silu(gate) * up_val).astype(jnp.bfloat16)
    terms = jnp.dot(hidden, down_full, preferred_element_type=jnp.float32)
    fed = lax.psum_scatter(
        terms.astype(jnp.bfloat16), "tp", scatter_dimension=0, tiled=True
    ).astype(jnp.float32)
    return (mixed_f + 0.5 * fed).astype(jnp.bfloat16)


NX = 2
NC = 2
LANES = 128


def ring_kernel(
    nz,
    res_ref, q_ref, k_ref, v_ref, cos_ref, sin_ref, qg_ref, kg_ref, ow_ref, ng_ref, g_ref, u_ref, d_ref,
    out_ref,
    g_own, u_own, d_own, k_own, k_all, v_all, g_all, u_all, d_all, q_s, att_s, proj, proj_in, normed_all,
    part, core_in, y_out, y_in, z_out, z_in, mixed_s,
    kz_s, kz_r, kx_s, kx_r, wz_s, wz_r, wx_s, wx_r, pj_s, pj_r,
    nz_s, nz_r, ny_s, ny_r, nc_s, nc_r, nf_s, nf_r,
    c_s, c_r, y_s, y_r, z_s, z_r, kf_s, af_s, ld_s,
):
    f32, bf16 = jnp.float32, jnp.bfloat16
    sp, tp = lax.axis_index("sp"), lax.axis_index("tp")
    z, x = sp // NX, sp % NX
    y, c = tp // NC, tp % NC
    ntp = 2 * NC
    tok = q_ref.shape[0]
    hd = k_ref.shape[1]
    heads = q_ref.shape[1] // hd
    rows = res_ref.shape[0]
    wide = res_ref.shape[1]
    drows = g_ref.shape[0]
    unit = g_all.shape[1]

    def at_z(zz):
        return (zz * NX + x, tp)

    x_peer = (z * NX + (1 - x), tp)
    y_peer = (sp, (1 - y) * NC + c)
    c_peer = (sp, y * NC + (1 - c))

    def up(d):
        return lax.rem(z + d, nz)

    def down(d):
        return lax.rem(z + nz - d, nz)

    def rc(src, dst, ss, rs, dev):
        return pltpu.make_async_remote_copy(
            src_ref=src, dst_ref=dst, send_sem=ss, recv_sem=rs, device_id=dev,
            device_id_type=pl.DeviceIdType.MESH,
        )

    units = g_ref.shape[1]
    loads = (
        pltpu.make_async_copy(g_ref, g_own.at[:, pl.ds(0, units)], ld_s.at[0]),
        pltpu.make_async_copy(u_ref, u_own.at[:, pl.ds(0, units)], ld_s.at[1]),
        pltpu.make_async_copy(d_ref, d_own.at[pl.ds(0, units), :], ld_s.at[2]),
    )
    for op in loads:
        op.start()
    extra = g_own.shape[1] - units
    if extra:
        g_own[:, units:] = jnp.zeros((drows, extra), bf16)
        u_own[:, units:] = jnp.zeros((drows, extra), bf16)
        d_own[units:, :] = jnp.zeros((extra, d_own.shape[1]), bf16)

    def near(i):
        i = jnp.int32(i)
        ahead = jnp.where(i == 1, 0, i)
        inner = jnp.where(z == 1, ahead, nz - 1 - ahead)
        return jnp.where(i == 0, z, jnp.where(z == 0, i, jnp.where(z == nz - 1, nz - 1 - i, inner)))

    barrier = pltpu.get_barrier_semaphore()
    peers = [at_z(up(d)) for d in range(1, nz)] + [x_peer]
    peers += [(sp, lax.rem(tp + e, ntp)) for e in range(1, ntp)]
    for dev in peers:
        pl.semaphore_signal(barrier, inc=1, device_id=dev, device_id_type=pl.DeviceIdType.MESH)
    pl.semaphore_wait(barrier, len(peers))

    lane = lax.broadcasted_iota(jnp.int32, (tok, hd), 1)
    low = (lane % (hd // 2)) < (hd // 4)
    cosine, sine = cos_ref[...], sin_ref[...]

    def prepare(raw, gain):
        vec = raw.astype(f32)
        vec = vec * lax.rsqrt(jnp.mean(vec * vec, axis=-1, keepdims=True) + EPS) * gain
        swapped = jnp.where(low, pltpu.roll(vec, hd - hd // 4, 1), pltpu.roll(vec, hd // 4, 1))
        return (vec * cosine + swapped * sine).astype(bf16)

    def tok_rows(s):
        return pl.ds(pl.multiple_of(s * tok, tok), tok)

    def w_rows(s):
        return pl.ds(pl.multiple_of(s * drows, drows), drows)

    def w_cols(zz):
        return pl.ds(pl.multiple_of(zz * unit, unit), unit)

    k_new = prepare(k_ref[...], kg_ref[...])
    k_own[...] = k_new
    mine = tok_rows(sp)
    k_all[mine, :] = k_new
    v_all[mine, :] = v_ref[...]

    def line_dev(way):
        return at_z(lax.clamp(0, z + way, nz - 1))

    def onward(t):
        way = jnp.where(t < z, 1, -1)
        inside = jnp.logical_and(z + way >= 0, z + way < nz)
        return at_z(lax.clamp(0, z + way, nz - 1)), inside

    ways = ((1, z < nz - 1), (-1, z > 0))

    def kv_out(w, way):
        return (
            rc(k_own, k_all.at[mine, :], kz_s.at[0, w], kz_r.at[0, z], line_dev(way)),
            rc(v_ref, v_all.at[mine, :], kz_s.at[1, w], kz_r.at[1, z], line_dev(way)),
        )

    def kv_in(t, i, dev):
        theirs = tok_rows(t * NX + x)
        return (
            rc(k_all.at[theirs, :], k_all.at[theirs, :], kf_s.at[0, i], kz_r.at[0, t], dev),
            rc(v_all.at[theirs, :], v_all.at[theirs, :], kf_s.at[1, i], kz_r.at[1, t], dev),
        )

    def starts(ops):
        for op in ops:
            op.start()

    def sent(ops):
        for op in ops:
            op.wait_send()

    for w, (way, ok) in enumerate(ways):
        pl.when(ok)(functools.partial(starts, kv_out(w, way)))
    kx = [(
        rc(k_own, k_all.at[mine, :], kx_s.at[0, 0], kx_r.at[0, 0], x_peer),
        rc(v_ref, v_all.at[mine, :], kx_s.at[1, 0], kx_r.at[1, 0], x_peer),
    )]
    for op in kx[0]:
        op.start()

    def pieces(zz, s_sem, r_sem, i, dev):
        return (
            rc(g_own.at[:, w_cols(zz)], g_all.at[w_rows(sp), :], s_sem.at[0, i], r_sem.at[0, i], dev),
            rc(u_own.at[:, w_cols(zz)], u_all.at[w_rows(sp), :], s_sem.at[1, i], r_sem.at[1, i], dev),
            rc(d_own.at[w_cols(zz), :], d_all.at[sp], s_sem.at[2, i], r_sem.at[2, i], dev),
        )

    for op in loads:
        op.wait()
    wz = []
    for d in range(1, nz):
        wz.append(pieces(up(d), wz_s, wz_r, d, at_z(up(d))))
        for op in wz[-1]:
            op.start()

    for h in range(heads):
        q_s[h] = prepare(q_ref[:, h * hd:(h + 1) * hd], qg_ref[...])
    g_all[w_rows(sp), :] = g_own[:, w_cols(z)]
    u_all[w_rows(sp), :] = u_own[:, w_cols(z)]
    d_all[sp] = d_own[w_cols(z), :]

    for i in range(1, nz):
        t = near(i)
        dev, inside = onward(t)
        ops = kv_in(t, i, dev)
        for op in ops:
            op.wait_recv()
        pl.when(inside)(functools.partial(starts, ops))
        theirs = tok_rows(t * NX + x)
        kx.append((
            rc(k_all.at[theirs, :], k_all.at[theirs, :], kx_s.at[0, i], kx_r.at[0, i], x_peer),
            rc(v_all.at[theirs, :], v_all.at[theirs, :], kx_s.at[1, i], kx_r.at[1, i], x_peer),
        ))
        starts(kx[-1])
    wx = [pieces(z, wx_s, wx_r, 0, x_peer)]
    for op in wx[0]:
        op.start()
    for pair in kx:
        for op in pair:
            op.wait_recv()

    scale = hd ** (-0.5)
    for h in range(heads):
        scores = lax.dot_general(
            q_s[h], k_all[...], (((1,), (1,)), ((), ())), preferred_element_type=f32
        )
        top = jnp.max(scores, axis=-1, keepdims=True)
        expo = jnp.exp((scores - top) * scale)
        total = jnp.sum(expo, axis=-1, keepdims=True)
        summed = jnp.dot(expo.astype(bf16), v_all[...], preferred_element_type=f32)
        att_s[:, h * hd:(h + 1) * hd] = (summed / total).astype(bf16)

    step = wide // 4
    for i in range(4):
        cols = slice(i * step, (i + 1) * step)
        prod = jnp.dot(att_s[...], ow_ref[:, cols], preferred_element_type=f32)
        proj[:, :, cols] = prod.astype(bf16).reshape(ntp, rows, step)
    pj = []
    for e in range(1, ntp):
        to = lax.rem(tp + e, ntp)
        pj.append(rc(proj.at[to], proj_in.at[e - 1], pj_s.at[e], pj_r.at[e], (sp, to)))
        pj[-1].start()

    def forward_weights(d):
        for op in wz[d - 1]:
            op.wait_recv()
        s = down(d) * NX + x
        wx.append((
            rc(g_all.at[w_rows(s), :], g_all.at[w_rows(s), :], wx_s.at[0, d], wx_r.at[0, d], x_peer),
            rc(u_all.at[w_rows(s), :], u_all.at[w_rows(s), :], wx_s.at[1, d], wx_r.at[1, d], x_peer),
            rc(d_all.at[s], d_all.at[s], wx_s.at[2, d], wx_r.at[2, d], x_peer),
        ))
        for op in wx[-1]:
            op.start()

    forward_weights(1)
    for op in pj:
        op.wait_recv()
    projected = proj[tp].astype(f32)
    for e in range(1, ntp):
        projected = projected + proj_in[e - 1].astype(f32)
    mixed = (res_ref[...].astype(f32) + projected).astype(bf16)
    mixed_s[...] = mixed
    mixed_f = mixed.astype(f32)
    normed = (
        mixed_f * lax.rsqrt(jnp.mean(mixed_f * mixed_f, axis=-1, keepdims=True) + EPS) * ng_ref[...]
    ).astype(bf16)
    own = z * ntp + tp
    normed_all[own] = normed

    mine_blk = normed_all.at[own]

    def row_out(w, way):
        return rc(mine_blk, mine_blk, nz_s.at[w], nz_r.at[z], line_dev(way))

    def row_in(t, i, dev):
        blk = normed_all.at[t * ntp + tp]
        return rc(blk, blk, af_s.at[i], nz_r.at[t], dev)

    def y_copy(t):
        blk = normed_all.at[t * ntp + tp]
        return rc(blk, blk, ny_s.at[t], ny_r.at[t], y_peer)

    def c_copy(t):
        blk = normed_all.at[t * ntp + tp]
        return rc(blk, blk, nc_s.at[t], nc_r.at[t], c_peer)

    def f_copy(t):
        blk = normed_all.at[t * ntp + (1 - y) * NC + c]
        return rc(blk, blk, nf_s.at[t], nf_r.at[t], c_peer)

    def pass_on(t):
        y_copy(t).start()
        c_copy(t).start()

    def pass_over(t):
        y_copy(t).wait_recv()
        f_copy(t).start()

    for w, (way, ok) in enumerate(ways):
        pl.when(ok)(row_out(w, way).start)
    pass_on(z)
    forward_weights(2)
    pass_over(z)
    forward_weights(3)
    for i in range(1, nz):
        t = near(i)
        dev, inside = onward(t)
        op = row_in(t, i, dev)
        op.wait_recv()
        pl.when(inside)(op.start)
        pass_on(t)
        if i > 1:
            pass_over(near(i - 1))
    for ops in wx:
        for op in ops:
            op.wait_recv()

    def core_ops(t, j):
        b = t * ntp + j * NC + (1 - c)
        return rc(part.at[b], core_in.at[t, j], c_s.at[t, j], c_r.at[t, j], c_peer)

    def y_op(t):
        return rc(y_out.at[t], y_in.at[t], y_s.at[t], y_r.at[t], y_peer)

    def y_stage(t):
        for j in range(2):
            core_ops(t, j).wait_recv()
        b = t * ntp + (1 - y) * NC + c
        y_out[t] = (part[b].astype(f32) + core_in[t, 1 - y].astype(f32)).astype(bf16)
        y_op(t).start()

    cols_each = d_all.shape[2]

    def tile(i, carry):
        t = near(i)

        @pl.when(i == nz - 2)
        def _():
            pass_over(near(nz - 1))

        c_copy(t).wait_recv()
        f_copy(t).wait_recv()
        x_t = normed_all[pl.ds(t * ntp, ntp)].reshape(ntp * rows, wide)
        gate = jnp.dot(x_t, g_all[...], preferred_element_type=f32)
        up_val = jnp.dot(x_t, u_all[...], preferred_element_type=f32)
        hidden = (gate / (1.0 + jnp.exp(-gate)) * up_val).astype(bf16)
        for s in range(d_all.shape[0]):
            r = jnp.dot(hidden, d_all[s], preferred_element_type=f32).astype(bf16)
            part[pl.ds(t * ntp, ntp), :, s * cols_each:(s + 1) * cols_each] = r.reshape(ntp, rows, cols_each)
        for j in range(2):
            core_ops(t, j).start()

        @pl.when(i > 1)
        def _():
            y_stage(near(i - 1))

        return carry

    lax.fori_loop(0, nz, tile, 0)

    y_stage(near(nz - 1))
    y_stage(z)

    def summed_tile(t):
        return part[t * ntp + tp].astype(f32) + core_in[t, y].astype(f32) + y_in[t].astype(f32)

    def z_op(i):
        return rc(z_out.at[i], z_in.at[z], z_s.at[i], z_r.at[z], at_z(near(i)))

    for i in range(1, nz):
        t = near(i)
        y_op(t).wait_recv()
        z_out[i] = summed_tile(t).astype(bf16)
        z_op(i).start()
    y_op(z).wait_recv()
    fed = summed_tile(z)
    for i in range(1, nz):
        t = near(i)
        rc(z_out.at[i], z_in.at[t], z_s.at[i], z_r.at[t], at_z(t)).wait_recv()
        fed = fed + z_in[t].astype(f32)
    out_ref[...] = (mixed_s[...].astype(f32) + 0.5 * fed).astype(bf16)

    for ops in kx + wz + wx:
        sent(ops)
    sent(pj)
    for w, (way, ok) in enumerate(ways):
        pl.when(ok)(functools.partial(sent, kv_out(w, way) + (row_out(w, way),)))
    for i in range(nz):
        t = near(i)
        sent((y_copy(t), c_copy(t), f_copy(t), core_ops(t, 0), core_ops(t, 1), y_op(t)))
        if i:
            dev, inside = onward(t)
            pl.when(inside)(functools.partial(sent, kv_in(t, i, dev) + (row_in(t, i, dev),)))
            z_op(i).wait_send()


def ring_device(
    nsp,
    residual_in, queries, keys_raw, values_raw, query_gain, key_gain, out_weight, norm_gain,
    gate_weight, up_weight, down_weight,
):
    bf16 = jnp.bfloat16
    nz = nsp // NX
    tok = queries.shape[0]
    hd = query_gain.shape[0]
    heads = queries.shape[1] // hd
    rows, wide = residual_in.shape
    drows, units = gate_weight.shape
    ntp = tok // rows
    unit = -(-units // (nz * LANES)) * LANES
    half = hd // 2
    positions = lax.axis_index("sp") * tok + jnp.arange(tok, dtype=jnp.int32)
    freqs = THETA ** (-jnp.arange(0, half, 2, dtype=jnp.float32) / half)
    row_ang = (positions // GRID_W).astype(jnp.float32)[:, None] * freqs
    col_ang = (positions % GRID_W).astype(jnp.float32)[:, None] * freqs
    angles = jnp.concatenate([row_ang, row_ang, col_ang, col_ang], axis=-1)
    sign = jnp.where(jnp.arange(hd) % half < half // 2, -1.0, 1.0)
    cosine, sine = jnp.cos(angles), jnp.sin(angles) * sign
    dma = pltpu.SemaphoreType.DMA
    vm = pltpu.VMEM
    blk = (rows, wide)
    scratch = [
        vm((drows, nz * unit), bf16), vm((drows, nz * unit), bf16), vm((nz * unit, down_weight.shape[1]), bf16),
        vm((tok, hd), bf16), vm((nsp * tok, hd), bf16), vm((nsp * tok, hd), bf16),
        vm((nsp * drows, unit), bf16), vm((nsp * drows, unit), bf16), vm((nsp, unit, down_weight.shape[1]), bf16),
        vm((heads, tok, hd), bf16), vm((tok, heads * hd), bf16),
        vm((ntp,) + blk, bf16), vm((ntp - 1,) + blk, bf16), vm((nz * ntp,) + blk, bf16),
        vm((nz * ntp,) + blk, bf16), vm((nz, 2) + blk, bf16), vm((nz,) + blk, bf16), vm((nz,) + blk, bf16),
        vm((nz,) + blk, bf16), vm((nz,) + blk, bf16), vm(blk, bf16),
        dma((2, nz)), dma((2, nz)), dma((2, nz)), dma((2, nz)),
        dma((3, nz)), dma((3, nz)), dma((3, nz)), dma((3, nz)),
        dma((ntp,)), dma((ntp,)),
    ] + [dma((nz,)) for _ in range(8)] + [
        dma((nz, 2)), dma((nz, 2)), dma((nz,)), dma((nz,)), dma((nz,)), dma((nz,)),
        dma((2, nz)), dma((nz,)), dma((3,)),
    ]
    return pl.pallas_call(
        functools.partial(ring_kernel, nz),
        out_shape=jax.ShapeDtypeStruct(blk, bf16),
        in_specs=[pl.BlockSpec(memory_space=pltpu.VMEM)] * 10 + [pl.BlockSpec(memory_space=pl.ANY)] * 3,
        out_specs=pl.BlockSpec(memory_space=pltpu.VMEM),
        scratch_shapes=scratch,
        compiler_params=pltpu.CompilerParams(
            collective_id=0, has_side_effects=True, vmem_limit_bytes=60 * 1024 * 1024
        ),
    )(
        residual_in, queries, keys_raw, values_raw, cosine, sine, query_gain[None], key_gain[None],
        out_weight, norm_gain[None], gate_weight, up_weight, down_weight,
    )


def solution(mesh):
    nsp, ntp = mesh.shape["sp"], mesh.shape["tp"]

    def per_device(*arrays):
        residual_in, queries, keys_raw = arrays[:3]
        hd = arrays[4].shape[0]
        small = (
            nsp == 8 and ntp == 2 * NC and keys_raw.shape[1] == hd
            and queries.shape[0] == ntp * residual_in.shape[0]
            and arrays[8].shape[0] % LANES == 0 and queries.shape[0] <= 256
        )
        if small:
            return ring_device(nsp, *arrays)
        return plain_device(*arrays)

    placed = (
        P(("sp", "tp"), None),
        P("sp", "tp"),
        P("sp", "tp"),
        P("sp", "tp"),
        P(),
        P(),
        P("tp", None),
        P(),
        P("sp", "tp"),
        P("sp", "tp"),
        P("tp", "sp"),
    )
    return jax.shard_map(
        per_device, mesh=mesh, in_specs=placed, out_specs=P(("sp", "tp"), None), check_vma=False
    )
```

```python
import jax
import jax.numpy as jnp
from jax import lax
from jax.experimental import pallas as pl
from jax.experimental.pallas import tpu as pltpu
import functools
from jax.sharding import PartitionSpec as P

GRID_W = 64


EPS = 1e-06
THETA = 10000.0


def turn_half(part, angles):
    quarter = part.shape[-1] // 2
    cosine = jnp.cos(angles)[:, None, :]
    sine = jnp.sin(angles)[:, None, :]
    first = part[..., :quarter]
    second = part[..., quarter:]
    return part * cosine + jnp.concatenate([-second, first], axis=-1) * sine


def prepare_heads(raw, gain, positions, heads):
    count = raw.shape[0]
    head_dim = gain.shape[0]
    half = head_dim // 2
    vec = raw.astype(jnp.float32).reshape(count, heads, head_dim)
    vec = vec * lax.rsqrt(jnp.mean(vec * vec, axis=-1, keepdims=True) + EPS) * gain
    freqs = THETA ** (-jnp.arange(0, half, 2, dtype=jnp.float32) / half)
    row_ang = (positions // GRID_W).astype(jnp.float32)[:, None] * freqs
    col_ang = (positions % GRID_W).astype(jnp.float32)[:, None] * freqs
    row_ang = jnp.concatenate([row_ang, row_ang], axis=-1)
    col_ang = jnp.concatenate([col_ang, col_ang], axis=-1)
    turned = jnp.concatenate(
        [turn_half(vec[..., :half], row_ang), turn_half(vec[..., half:], col_ang)], axis=-1
    )
    return turned.astype(jnp.bfloat16)


def plain_device(
    residual_in,
    queries,
    keys_raw,
    values_raw,
    query_gain,
    key_gain,
    out_weight,
    norm_gain,
    gate_weight,
    up_weight,
    down_weight,
):
    tok = queries.shape[0]
    head_dim = query_gain.shape[0]
    local_heads = queries.shape[1] // head_dim
    local_kv = keys_raw.shape[1] // head_dim
    group = local_heads // local_kv
    gate_full, up_full = (
        lax.all_gather(gate_weight, "sp", axis=0, tiled=True),
        lax.all_gather(up_weight, "sp", axis=0, tiled=True),
    )
    down_full = lax.all_gather(down_weight, "sp", axis=1, tiled=True)
    positions = lax.axis_index("sp") * tok + jnp.arange(tok, dtype=jnp.int32)
    q_rot = prepare_heads(queries, query_gain, positions, local_heads).reshape(
        tok, local_kv, group, head_dim
    )
    k_rot = prepare_heads(keys_raw, key_gain, positions, local_kv)
    vals = values_raw.reshape(tok, local_kv, head_dim)
    start_state = (
        jnp.full((tok, local_kv, group), -jnp.inf, jnp.float32),
        jnp.zeros((tok, local_kv, group), jnp.float32),
        jnp.zeros((tok, local_kv, group, head_dim), jnp.float32),
    )
    carry = start_state
    k_piece = lax.all_gather(k_rot, "sp", axis=0, tiled=True)
    v_piece = lax.all_gather(vals, "sp", axis=0, tiled=True)
    length = k_piece.shape[0]
    shards = length // tok
    per_step = max(1, 2048 // tok)
    factor = max((d for d in range(1, shards + 1) if shards % d == 0 and d <= per_step))
    span = factor * tok
    k_blocks = k_piece.reshape(length // span, span, local_kv, head_dim)
    v_blocks = v_piece.reshape(length // span, span, local_kv, head_dim)

    def step(state, blocks):
        top, total, summed = state
        k_blk, v_blk = blocks
        scores = jnp.einsum(
            "qkgd,skd->qkgs", q_rot, k_blk, preferred_element_type=jnp.float32
        ) * head_dim ** (-0.5)
        new_top = jnp.maximum(top, jnp.max(scores, axis=-1))
        shrink = jnp.exp(top - new_top)
        expo = jnp.exp(scores - new_top[..., None])
        total = total * shrink + jnp.sum(expo, axis=-1)
        summed = summed * shrink[..., None] + jnp.einsum(
            "qkgs,skd->qkgd", expo.astype(jnp.bfloat16), v_blk, preferred_element_type=jnp.float32
        )
        return ((new_top, total, summed), None)

    carry, _ = lax.scan(step, carry, (k_blocks, v_blocks))
    top, total, summed = carry
    attended = (summed / total[..., None]).astype(jnp.bfloat16).reshape(tok, local_heads * head_dim)
    projected = lax.psum_scatter(
        jnp.dot(attended, out_weight, preferred_element_type=jnp.float32).astype(jnp.bfloat16),
        "tp",
        scatter_dimension=0,
        tiled=True,
    ).astype(jnp.float32)
    mixed = (residual_in.astype(jnp.float32) + projected).astype(jnp.bfloat16)
    mixed_f = mixed.astype(jnp.float32)
    normed = (
        mixed_f * lax.rsqrt(jnp.mean(mixed_f * mixed_f, axis=-1, keepdims=True) + EPS) * norm_gain
    ).astype(jnp.bfloat16)
    whole_rows = lax.all_gather(normed, "tp", axis=0, tiled=True)
    gate = jnp.dot(whole_rows, gate_full, preferred_element_type=jnp.float32)
    up_val = jnp.dot(whole_rows, up_full, preferred_element_type=jnp.float32)
    hidden = (jax.nn.silu(gate) * up_val).astype(jnp.bfloat16)
    terms = jnp.dot(hidden, down_full, preferred_element_type=jnp.float32)
    fed = lax.psum_scatter(
        terms.astype(jnp.bfloat16), "tp", scatter_dimension=0, tiled=True
    ).astype(jnp.float32)
    return (mixed_f + 0.5 * fed).astype(jnp.bfloat16)


NX = 2
NC = 2
LANES = 128


def ring_kernel(
    nz,
    res_ref, q_ref, k_ref, v_ref, cos_ref, sin_ref, qg_ref, kg_ref, ow_ref, ng_ref, g_ref, u_ref, d_ref,
    out_ref,
    g_own, u_own, d_own, k_own, k_all, v_all, g_all, u_all, d_all, q_s, att_s, proj, proj_in, normed_all,
    part, core_in, y_out, y_in, z_out, z_in, mixed_s,
    kz_s, kz_r, kx_s, kx_r, wz_s, wz_r, wx_s, wx_r, pj_s, pj_r,
    nz_s, nz_r, ny_s, ny_r, nc_s, nc_r, nf_s, nf_r,
    c_s, c_r, y_s, y_r, z_s, z_r, af_s, ld_s,
):
    f32, bf16 = jnp.float32, jnp.bfloat16
    sp, tp = lax.axis_index("sp"), lax.axis_index("tp")
    z, x = sp // NX, sp % NX
    y, c = tp // NC, tp % NC
    ntp = 2 * NC
    tok = q_ref.shape[0]
    hd = k_ref.shape[1]
    heads = q_ref.shape[1] // hd
    rows = res_ref.shape[0]
    wide = res_ref.shape[1]
    drows = g_ref.shape[0]
    unit = g_all.shape[1]

    def at_z(zz):
        return (zz * NX + x, tp)

    x_peer = (z * NX + (1 - x), tp)
    y_peer = (sp, (1 - y) * NC + c)
    c_peer = (sp, y * NC + (1 - c))

    def up(d):
        return lax.rem(z + d, nz)

    def down(d):
        return lax.rem(z + nz - d, nz)

    def rc(src, dst, ss, rs, dev):
        return pltpu.make_async_remote_copy(
            src_ref=src, dst_ref=dst, send_sem=ss, recv_sem=rs, device_id=dev,
            device_id_type=pl.DeviceIdType.MESH,
        )

    units = g_ref.shape[1]
    loads = (
        pltpu.make_async_copy(g_ref, g_own.at[:, pl.ds(0, units)], ld_s.at[0]),
        pltpu.make_async_copy(u_ref, u_own.at[:, pl.ds(0, units)], ld_s.at[1]),
        pltpu.make_async_copy(d_ref, d_own.at[pl.ds(0, units), :], ld_s.at[2]),
    )
    for op in loads:
        op.start()
    extra = g_own.shape[1] - units
    if extra:
        g_own[:, units:] = jnp.zeros((drows, extra), bf16)
        u_own[:, units:] = jnp.zeros((drows, extra), bf16)
        d_own[units:, :] = jnp.zeros((extra, d_own.shape[1]), bf16)

    def near(i):
        i = jnp.int32(i)
        ahead = jnp.where(i == 1, 0, i)
        inner = jnp.where(z == 1, ahead, nz - 1 - ahead)
        return jnp.where(i == 0, z, jnp.where(z == 0, i, jnp.where(z == nz - 1, nz - 1 - i, inner)))

    barrier = pltpu.get_barrier_semaphore()
    peers = [at_z(up(d)) for d in range(1, nz)] + [x_peer]
    peers += [(sp, lax.rem(tp + e, ntp)) for e in range(1, ntp)]
    for dev in peers:
        pl.semaphore_signal(barrier, inc=1, device_id=dev, device_id_type=pl.DeviceIdType.MESH)
    pl.semaphore_wait(barrier, len(peers))

    lane = lax.broadcasted_iota(jnp.int32, (tok, hd), 1)
    low = (lane % (hd // 2)) < (hd // 4)
    cosine, sine = cos_ref[...], sin_ref[...]

    def prepare(raw, gain):
        vec = raw.astype(f32)
        vec = vec * lax.rsqrt(jnp.mean(vec * vec, axis=-1, keepdims=True) + EPS) * gain
        swapped = jnp.where(low, pltpu.roll(vec, hd - hd // 4, 1), pltpu.roll(vec, hd // 4, 1))
        return (vec * cosine + swapped * sine).astype(bf16)

    def tok_rows(s):
        return pl.ds(pl.multiple_of(s * tok, tok), tok)

    def w_rows(s):
        return pl.ds(pl.multiple_of(s * drows, drows), drows)

    def w_cols(zz):
        return pl.ds(pl.multiple_of(zz * unit, unit), unit)

    k_new = prepare(k_ref[...], kg_ref[...])
    k_own[...] = k_new
    mine = tok_rows(sp)
    k_all[mine, :] = k_new
    v_all[mine, :] = v_ref[...]

    def line_dev(way):
        return at_z(lax.clamp(0, z + way, nz - 1))

    def onward(t):
        way = jnp.where(t < z, 1, -1)
        inside = jnp.logical_and(z + way >= 0, z + way < nz)
        return at_z(lax.clamp(0, z + way, nz - 1)), inside

    ways = ((1, z < nz - 1), (-1, z > 0))

    def kv_out(i):
        dev = at_z(near(i))
        return (
            rc(k_own, k_all.at[mine, :], kz_s.at[0, i], kz_r.at[0, z], dev),
            rc(v_ref, v_all.at[mine, :], kz_s.at[1, i], kz_r.at[1, z], dev),
        )

    def kv_in(i):
        t = near(i)
        theirs = tok_rows(t * NX + x)
        return (
            rc(k_own, k_all.at[theirs, :], kz_s.at[0, i], kz_r.at[0, t], at_z(t)),
            rc(v_ref, v_all.at[theirs, :], kz_s.at[1, i], kz_r.at[1, t], at_z(t)),
        )

    def starts(ops):
        for op in ops:
            op.start()

    def sent(ops):
        for op in ops:
            op.wait_send()

    for i in range(nz - 1, 0, -1):
        starts(kv_out(i))
    kx = [(
        rc(k_own, k_all.at[mine, :], kx_s.at[0, 0], kx_r.at[0, 0], x_peer),
        rc(v_ref, v_all.at[mine, :], kx_s.at[1, 0], kx_r.at[1, 0], x_peer),
    )]
    for op in kx[0]:
        op.start()

    def pieces(zz, s_sem, r_sem, i, dev):
        return (
            rc(g_own.at[:, w_cols(zz)], g_all.at[w_rows(sp), :], s_sem.at[0, i], r_sem.at[0, i], dev),
            rc(u_own.at[:, w_cols(zz)], u_all.at[w_rows(sp), :], s_sem.at[1, i], r_sem.at[1, i], dev),
            rc(d_own.at[w_cols(zz), :], d_all.at[sp], s_sem.at[2, i], r_sem.at[2, i], dev),
        )

    for op in loads:
        op.wait()
    wz = []
    for d in range(1, nz):
        wz.append(pieces(up(d), wz_s, wz_r, d, at_z(up(d))))
        for op in wz[-1]:
            op.start()

    for h in range(heads):
        q_s[h] = prepare(q_ref[:, h * hd:(h + 1) * hd], qg_ref[...])
    g_all[w_rows(sp), :] = g_own[:, w_cols(z)]
    u_all[w_rows(sp), :] = u_own[:, w_cols(z)]
    d_all[sp] = d_own[w_cols(z), :]

    for i in range(1, nz):
        t = near(i)
        for op in kv_in(i):
            op.wait_recv()
        theirs = tok_rows(t * NX + x)
        kx.append((
            rc(k_all.at[theirs, :], k_all.at[theirs, :], kx_s.at[0, i], kx_r.at[0, i], x_peer),
            rc(v_all.at[theirs, :], v_all.at[theirs, :], kx_s.at[1, i], kx_r.at[1, i], x_peer),
        ))
        starts(kx[-1])
    wx = [pieces(z, wx_s, wx_r, 0, x_peer)]
    for op in wx[0]:
        op.start()
    for pair in kx:
        for op in pair:
            op.wait_recv()

    scale = hd ** (-0.5)
    for h in range(heads):
        scores = lax.dot_general(
            q_s[h], k_all[...], (((1,), (1,)), ((), ())), preferred_element_type=f32
        )
        top = jnp.max(scores, axis=-1, keepdims=True)
        expo = jnp.exp((scores - top) * scale)
        total = jnp.sum(expo, axis=-1, keepdims=True)
        summed = jnp.dot(expo.astype(bf16), v_all[...], preferred_element_type=f32)
        att_s[:, h * hd:(h + 1) * hd] = (summed / total).astype(bf16)

    step = wide // 4
    for i in range(4):
        cols = slice(i * step, (i + 1) * step)
        prod = jnp.dot(att_s[...], ow_ref[:, cols], preferred_element_type=f32)
        proj[:, :, cols] = prod.astype(bf16).reshape(ntp, rows, step)
    pj = []
    for e in range(1, ntp):
        to = lax.rem(tp + e, ntp)
        pj.append(rc(proj.at[to], proj_in.at[e - 1], pj_s.at[e], pj_r.at[e], (sp, to)))
        pj[-1].start()

    def forward_weights(d):
        for op in wz[d - 1]:
            op.wait_recv()
        s = down(d) * NX + x
        wx.append((
            rc(g_all.at[w_rows(s), :], g_all.at[w_rows(s), :], wx_s.at[0, d], wx_r.at[0, d], x_peer),
            rc(u_all.at[w_rows(s), :], u_all.at[w_rows(s), :], wx_s.at[1, d], wx_r.at[1, d], x_peer),
            rc(d_all.at[s], d_all.at[s], wx_s.at[2, d], wx_r.at[2, d], x_peer),
        ))
        for op in wx[-1]:
            op.start()

    forward_weights(1)
    for op in pj:
        op.wait_recv()
    projected = proj[tp].astype(f32)
    for e in range(1, ntp):
        projected = projected + proj_in[e - 1].astype(f32)
    mixed = (res_ref[...].astype(f32) + projected).astype(bf16)
    mixed_s[...] = mixed
    mixed_f = mixed.astype(f32)
    normed = (
        mixed_f * lax.rsqrt(jnp.mean(mixed_f * mixed_f, axis=-1, keepdims=True) + EPS) * ng_ref[...]
    ).astype(bf16)
    own = z * ntp + tp
    normed_all[own] = normed

    mine_blk = normed_all.at[own]

    def row_out(w, way):
        return rc(mine_blk, mine_blk, nz_s.at[w], nz_r.at[z], line_dev(way))

    def row_in(t, i, dev):
        blk = normed_all.at[t * ntp + tp]
        return rc(blk, blk, af_s.at[i], nz_r.at[t], dev)

    def y_copy(t):
        blk = normed_all.at[t * ntp + tp]
        return rc(blk, blk, ny_s.at[t], ny_r.at[t], y_peer)

    def c_copy(t):
        blk = normed_all.at[t * ntp + tp]
        return rc(blk, blk, nc_s.at[t], nc_r.at[t], c_peer)

    def f_copy(t):
        blk = normed_all.at[t * ntp + (1 - y) * NC + c]
        return rc(blk, blk, nf_s.at[t], nf_r.at[t], c_peer)

    def pass_on(t):
        y_copy(t).start()
        c_copy(t).start()

    def pass_over(t):
        y_copy(t).wait_recv()
        f_copy(t).start()

    for w, (way, ok) in enumerate(ways):
        pl.when(ok)(row_out(w, way).start)
    pass_on(z)
    forward_weights(2)
    pass_over(z)
    forward_weights(3)
    for i in range(1, nz):
        t = near(i)
        dev, inside = onward(t)
        op = row_in(t, i, dev)
        op.wait_recv()
        pl.when(inside)(op.start)
        pass_on(t)
        if i > 1:
            pass_over(near(i - 1))
    for ops in wx:
        for op in ops:
            op.wait_recv()

    def core_ops(t, j):
        b = t * ntp + j * NC + (1 - c)
        return rc(part.at[b], core_in.at[t, j], c_s.at[t, j], c_r.at[t, j], c_peer)

    def y_op(t):
        return rc(y_out.at[t], y_in.at[t], y_s.at[t], y_r.at[t], y_peer)

    def y_stage(t):
        for j in range(2):
            core_ops(t, j).wait_recv()
        b = t * ntp + (1 - y) * NC + c
        y_out[t] = (part[b].astype(f32) + core_in[t, 1 - y].astype(f32)).astype(bf16)
        y_op(t).start()

    cols_each = d_all.shape[2]

    def tile(i, carry):
        t = near(i)

        @pl.when(i == nz - 2)
        def _():
            pass_over(near(nz - 1))

        c_copy(t).wait_recv()
        f_copy(t).wait_recv()
        x_t = normed_all[pl.ds(t * ntp, ntp)].reshape(ntp * rows, wide)
        gate = jnp.dot(x_t, g_all[...], preferred_element_type=f32)
        up_val = jnp.dot(x_t, u_all[...], preferred_element_type=f32)
        hidden = (gate / (1.0 + jnp.exp(-gate)) * up_val).astype(bf16)
        for s in range(d_all.shape[0]):
            r = jnp.dot(hidden, d_all[s], preferred_element_type=f32).astype(bf16)
            part[pl.ds(t * ntp, ntp), :, s * cols_each:(s + 1) * cols_each] = r.reshape(ntp, rows, cols_each)
        for j in range(2):
            core_ops(t, j).start()

        @pl.when(i > 1)
        def _():
            y_stage(near(i - 1))

        return carry

    lax.fori_loop(0, nz, tile, 0)

    y_stage(near(nz - 1))
    y_stage(z)

    def summed_tile(t):
        return part[t * ntp + tp].astype(f32) + core_in[t, y].astype(f32) + y_in[t].astype(f32)

    def z_op(i):
        return rc(z_out.at[i], z_in.at[z], z_s.at[i], z_r.at[z], at_z(near(i)))

    for i in range(1, nz):
        t = near(i)
        y_op(t).wait_recv()
        z_out[i] = summed_tile(t).astype(bf16)
        z_op(i).start()
    y_op(z).wait_recv()
    fed = summed_tile(z)
    for i in range(1, nz):
        t = near(i)
        rc(z_out.at[i], z_in.at[t], z_s.at[i], z_r.at[t], at_z(t)).wait_recv()
        fed = fed + z_in[t].astype(f32)
    out_ref[...] = (mixed_s[...].astype(f32) + 0.5 * fed).astype(bf16)

    for ops in kx + wz + wx:
        sent(ops)
    sent(pj)
    for w, (way, ok) in enumerate(ways):
        pl.when(ok)(row_out(w, way).wait_send)
    for i in range(nz):
        t = near(i)
        sent((y_copy(t), c_copy(t), f_copy(t), core_ops(t, 0), core_ops(t, 1), y_op(t)))
        if i:
            dev, inside = onward(t)
            pl.when(inside)(row_in(t, i, dev).wait_send)
            sent(kv_out(i))
            z_op(i).wait_send()


def ring_device(
    nsp,
    residual_in, queries, keys_raw, values_raw, query_gain, key_gain, out_weight, norm_gain,
    gate_weight, up_weight, down_weight,
):
    bf16 = jnp.bfloat16
    nz = nsp // NX
    tok = queries.shape[0]
    hd = query_gain.shape[0]
    heads = queries.shape[1] // hd
    rows, wide = residual_in.shape
    drows, units = gate_weight.shape
    ntp = tok // rows
    unit = -(-units // (nz * LANES)) * LANES
    half = hd // 2
    positions = lax.axis_index("sp") * tok + jnp.arange(tok, dtype=jnp.int32)
    freqs = THETA ** (-jnp.arange(0, half, 2, dtype=jnp.float32) / half)
    row_ang = (positions // GRID_W).astype(jnp.float32)[:, None] * freqs
    col_ang = (positions % GRID_W).astype(jnp.float32)[:, None] * freqs
    angles = jnp.concatenate([row_ang, row_ang, col_ang, col_ang], axis=-1)
    sign = jnp.where(jnp.arange(hd) % half < half // 2, -1.0, 1.0)
    cosine, sine = jnp.cos(angles), jnp.sin(angles) * sign
    dma = pltpu.SemaphoreType.DMA
    vm = pltpu.VMEM
    blk = (rows, wide)
    scratch = [
        vm((drows, nz * unit), bf16), vm((drows, nz * unit), bf16), vm((nz * unit, down_weight.shape[1]), bf16),
        vm((tok, hd), bf16), vm((nsp * tok, hd), bf16), vm((nsp * tok, hd), bf16),
        vm((nsp * drows, unit), bf16), vm((nsp * drows, unit), bf16), vm((nsp, unit, down_weight.shape[1]), bf16),
        vm((heads, tok, hd), bf16), vm((tok, heads * hd), bf16),
        vm((ntp,) + blk, bf16), vm((ntp - 1,) + blk, bf16), vm((nz * ntp,) + blk, bf16),
        vm((nz * ntp,) + blk, bf16), vm((nz, 2) + blk, bf16), vm((nz,) + blk, bf16), vm((nz,) + blk, bf16),
        vm((nz,) + blk, bf16), vm((nz,) + blk, bf16), vm(blk, bf16),
        dma((2, nz)), dma((2, nz)), dma((2, nz)), dma((2, nz)),
        dma((3, nz)), dma((3, nz)), dma((3, nz)), dma((3, nz)),
        dma((ntp,)), dma((ntp,)),
    ] + [dma((nz,)) for _ in range(8)] + [
        dma((nz, 2)), dma((nz, 2)), dma((nz,)), dma((nz,)), dma((nz,)), dma((nz,)),
        dma((nz,)), dma((3,)),
    ]
    return pl.pallas_call(
        functools.partial(ring_kernel, nz),
        out_shape=jax.ShapeDtypeStruct(blk, bf16),
        in_specs=[pl.BlockSpec(memory_space=pltpu.VMEM)] * 10 + [pl.BlockSpec(memory_space=pl.ANY)] * 3,
        out_specs=pl.BlockSpec(memory_space=pltpu.VMEM),
        scratch_shapes=scratch,
        compiler_params=pltpu.CompilerParams(
            collective_id=0, has_side_effects=True, vmem_limit_bytes=60 * 1024 * 1024
        ),
    )(
        residual_in, queries, keys_raw, values_raw, cosine, sine, query_gain[None], key_gain[None],
        out_weight, norm_gain[None], gate_weight, up_weight, down_weight,
    )


def solution(mesh):
    nsp, ntp = mesh.shape["sp"], mesh.shape["tp"]

    def per_device(*arrays):
        residual_in, queries, keys_raw = arrays[:3]
        hd = arrays[4].shape[0]
        small = (
            nsp == 8 and ntp == 2 * NC and keys_raw.shape[1] == hd
            and queries.shape[0] == ntp * residual_in.shape[0]
            and arrays[8].shape[0] % LANES == 0 and queries.shape[0] <= 256
        )
        if small:
            return ring_device(nsp, *arrays)
        return plain_device(*arrays)

    placed = (
        P(("sp", "tp"), None),
        P("sp", "tp"),
        P("sp", "tp"),
        P("sp", "tp"),
        P(),
        P(),
        P("tp", None),
        P(),
        P("sp", "tp"),
        P("sp", "tp"),
        P("tp", "sp"),
    )
    return jax.shard_map(
        per_device, mesh=mesh, in_specs=placed, out_specs=P(("sp", "tp"), None), check_vma=False
    )
```

```python
import jax
import jax.numpy as jnp
from jax import lax
from jax.experimental import pallas as pl
from jax.experimental.pallas import tpu as pltpu
import functools
from jax.sharding import PartitionSpec as P

GRID_W = 64


EPS = 1e-06
THETA = 10000.0


def turn_half(part, angles):
    quarter = part.shape[-1] // 2
    cosine = jnp.cos(angles)[:, None, :]
    sine = jnp.sin(angles)[:, None, :]
    first = part[..., :quarter]
    second = part[..., quarter:]
    return part * cosine + jnp.concatenate([-second, first], axis=-1) * sine


def prepare_heads(raw, gain, positions, heads):
    count = raw.shape[0]
    head_dim = gain.shape[0]
    half = head_dim // 2
    vec = raw.astype(jnp.float32).reshape(count, heads, head_dim)
    vec = vec * lax.rsqrt(jnp.mean(vec * vec, axis=-1, keepdims=True) + EPS) * gain
    freqs = THETA ** (-jnp.arange(0, half, 2, dtype=jnp.float32) / half)
    row_ang = (positions // GRID_W).astype(jnp.float32)[:, None] * freqs
    col_ang = (positions % GRID_W).astype(jnp.float32)[:, None] * freqs
    row_ang = jnp.concatenate([row_ang, row_ang], axis=-1)
    col_ang = jnp.concatenate([col_ang, col_ang], axis=-1)
    turned = jnp.concatenate(
        [turn_half(vec[..., :half], row_ang), turn_half(vec[..., half:], col_ang)], axis=-1
    )
    return turned.astype(jnp.bfloat16)


def plain_device(
    residual_in,
    queries,
    keys_raw,
    values_raw,
    query_gain,
    key_gain,
    out_weight,
    norm_gain,
    gate_weight,
    up_weight,
    down_weight,
):
    tok = queries.shape[0]
    head_dim = query_gain.shape[0]
    local_heads = queries.shape[1] // head_dim
    local_kv = keys_raw.shape[1] // head_dim
    group = local_heads // local_kv
    gate_full, up_full = (
        lax.all_gather(gate_weight, "sp", axis=0, tiled=True),
        lax.all_gather(up_weight, "sp", axis=0, tiled=True),
    )
    down_full = lax.all_gather(down_weight, "sp", axis=1, tiled=True)
    positions = lax.axis_index("sp") * tok + jnp.arange(tok, dtype=jnp.int32)
    q_rot = prepare_heads(queries, query_gain, positions, local_heads).reshape(
        tok, local_kv, group, head_dim
    )
    k_rot = prepare_heads(keys_raw, key_gain, positions, local_kv)
    vals = values_raw.reshape(tok, local_kv, head_dim)
    start_state = (
        jnp.full((tok, local_kv, group), -jnp.inf, jnp.float32),
        jnp.zeros((tok, local_kv, group), jnp.float32),
        jnp.zeros((tok, local_kv, group, head_dim), jnp.float32),
    )
    carry = start_state
    k_piece = lax.all_gather(k_rot, "sp", axis=0, tiled=True)
    v_piece = lax.all_gather(vals, "sp", axis=0, tiled=True)
    length = k_piece.shape[0]
    shards = length // tok
    per_step = max(1, 2048 // tok)
    factor = max((d for d in range(1, shards + 1) if shards % d == 0 and d <= per_step))
    span = factor * tok
    k_blocks = k_piece.reshape(length // span, span, local_kv, head_dim)
    v_blocks = v_piece.reshape(length // span, span, local_kv, head_dim)

    def step(state, blocks):
        top, total, summed = state
        k_blk, v_blk = blocks
        scores = jnp.einsum(
            "qkgd,skd->qkgs", q_rot, k_blk, preferred_element_type=jnp.float32
        ) * head_dim ** (-0.5)
        new_top = jnp.maximum(top, jnp.max(scores, axis=-1))
        shrink = jnp.exp(top - new_top)
        expo = jnp.exp(scores - new_top[..., None])
        total = total * shrink + jnp.sum(expo, axis=-1)
        summed = summed * shrink[..., None] + jnp.einsum(
            "qkgs,skd->qkgd", expo.astype(jnp.bfloat16), v_blk, preferred_element_type=jnp.float32
        )
        return ((new_top, total, summed), None)

    carry, _ = lax.scan(step, carry, (k_blocks, v_blocks))
    top, total, summed = carry
    attended = (summed / total[..., None]).astype(jnp.bfloat16).reshape(tok, local_heads * head_dim)
    projected = lax.psum_scatter(
        jnp.dot(attended, out_weight, preferred_element_type=jnp.float32).astype(jnp.bfloat16),
        "tp",
        scatter_dimension=0,
        tiled=True,
    ).astype(jnp.float32)
    mixed = (residual_in.astype(jnp.float32) + projected).astype(jnp.bfloat16)
    mixed_f = mixed.astype(jnp.float32)
    normed = (
        mixed_f * lax.rsqrt(jnp.mean(mixed_f * mixed_f, axis=-1, keepdims=True) + EPS) * norm_gain
    ).astype(jnp.bfloat16)
    whole_rows = lax.all_gather(normed, "tp", axis=0, tiled=True)
    gate = jnp.dot(whole_rows, gate_full, preferred_element_type=jnp.float32)
    up_val = jnp.dot(whole_rows, up_full, preferred_element_type=jnp.float32)
    hidden = (jax.nn.silu(gate) * up_val).astype(jnp.bfloat16)
    terms = jnp.dot(hidden, down_full, preferred_element_type=jnp.float32)
    fed = lax.psum_scatter(
        terms.astype(jnp.bfloat16), "tp", scatter_dimension=0, tiled=True
    ).astype(jnp.float32)
    return (mixed_f + 0.5 * fed).astype(jnp.bfloat16)


NX = 2
NC = 2
LANES = 128


def ring_kernel(
    nz,
    res_ref, q_ref, k_ref, v_ref, cos_ref, sin_ref, qg_ref, kg_ref, ow_ref, ng_ref, g_ref, u_ref, d_ref,
    out_ref,
    g_own, u_own, d_own, k_own, k_all, v_all, g_all, u_all, d_all, q_s, att_s, proj, proj_in, normed_all,
    part, core_in, y_out, y_in, z_out, z_in, mixed_s,
    kz_s, kz_r, kx_s, kx_r, wz_s, wz_r, wx_s, wx_r, pj_s, pj_r,
    nz_s, nz_r, ny_s, ny_r, nc_s, nc_r, nf_s, nf_r,
    c_s, c_r, y_s, y_r, z_s, z_r, af_s, ld_s,
):
    f32, bf16 = jnp.float32, jnp.bfloat16
    sp, tp = lax.axis_index("sp"), lax.axis_index("tp")
    z, x = sp // NX, sp % NX
    y, c = tp // NC, tp % NC
    ntp = 2 * NC
    tok = q_ref.shape[0]
    hd = k_ref.shape[1]
    heads = q_ref.shape[1] // hd
    rows = res_ref.shape[0]
    wide = res_ref.shape[1]
    drows = g_ref.shape[0]
    unit = g_all.shape[1]

    def at_z(zz):
        return (zz * NX + x, tp)

    x_peer = (z * NX + (1 - x), tp)
    y_peer = (sp, (1 - y) * NC + c)
    c_peer = (sp, y * NC + (1 - c))

    def up(d):
        return lax.rem(z + d, nz)

    def down(d):
        return lax.rem(z + nz - d, nz)

    def rc(src, dst, ss, rs, dev):
        return pltpu.make_async_remote_copy(
            src_ref=src, dst_ref=dst, send_sem=ss, recv_sem=rs, device_id=dev,
            device_id_type=pl.DeviceIdType.MESH,
        )

    units = g_ref.shape[1]
    loads = (
        pltpu.make_async_copy(g_ref, g_own.at[:, pl.ds(0, units)], ld_s.at[0]),
        pltpu.make_async_copy(u_ref, u_own.at[:, pl.ds(0, units)], ld_s.at[1]),
        pltpu.make_async_copy(d_ref, d_own.at[pl.ds(0, units), :], ld_s.at[2]),
    )
    for op in loads:
        op.start()
    extra = g_own.shape[1] - units
    if extra:
        g_own[:, units:] = jnp.zeros((drows, extra), bf16)
        u_own[:, units:] = jnp.zeros((drows, extra), bf16)
        d_own[units:, :] = jnp.zeros((extra, d_own.shape[1]), bf16)

    def near(i):
        i = jnp.int32(i)
        ahead = jnp.where(i == 1, 0, i)
        inner = jnp.where(z == 1, ahead, nz - 1 - ahead)
        return jnp.where(i == 0, z, jnp.where(z == 0, i, jnp.where(z == nz - 1, nz - 1 - i, inner)))

    barrier = pltpu.get_barrier_semaphore()
    peers = [at_z(up(d)) for d in range(1, nz)] + [x_peer]
    peers += [(sp, lax.rem(tp + e, ntp)) for e in range(1, ntp)]
    for dev in peers:
        pl.semaphore_signal(barrier, inc=1, device_id=dev, device_id_type=pl.DeviceIdType.MESH)
    pl.semaphore_wait(barrier, len(peers))

    lane = lax.broadcasted_iota(jnp.int32, (tok, hd), 1)
    low = (lane % (hd // 2)) < (hd // 4)
    cosine, sine = cos_ref[...], sin_ref[...]

    def prepare(raw, gain):
        vec = raw.astype(f32)
        vec = vec * lax.rsqrt(jnp.mean(vec * vec, axis=-1, keepdims=True) + EPS) * gain
        swapped = jnp.where(low, pltpu.roll(vec, hd - hd // 4, 1), pltpu.roll(vec, hd // 4, 1))
        return (vec * cosine + swapped * sine).astype(bf16)

    def tok_rows(s):
        return pl.ds(pl.multiple_of(s * tok, tok), tok)

    def w_rows(s):
        return pl.ds(pl.multiple_of(s * drows, drows), drows)

    def w_cols(zz):
        return pl.ds(pl.multiple_of(zz * unit, unit), unit)

    k_new = prepare(k_ref[...], kg_ref[...])
    k_own[...] = k_new
    mine = tok_rows(sp)
    k_all[mine, :] = k_new
    v_all[mine, :] = v_ref[...]

    def line_dev(way):
        return at_z(lax.clamp(0, z + way, nz - 1))

    def onward(t):
        way = jnp.where(t < z, 1, -1)
        inside = jnp.logical_and(z + way >= 0, z + way < nz)
        return at_z(lax.clamp(0, z + way, nz - 1)), inside

    ways = ((1, z < nz - 1), (-1, z > 0))

    def kv_out(i):
        dev = at_z(near(i))
        return (
            rc(k_own, k_all.at[mine, :], kz_s.at[0, i], kz_r.at[0, z], dev),
            rc(v_ref, v_all.at[mine, :], kz_s.at[1, i], kz_r.at[1, z], dev),
        )

    def kv_in(i):
        t = near(i)
        theirs = tok_rows(t * NX + x)
        return (
            rc(k_own, k_all.at[theirs, :], kz_s.at[0, i], kz_r.at[0, t], at_z(t)),
            rc(v_ref, v_all.at[theirs, :], kz_s.at[1, i], kz_r.at[1, t], at_z(t)),
        )

    def starts(ops):
        for op in ops:
            op.start()

    def sent(ops):
        for op in ops:
            op.wait_send()

    for i in range(nz - 1, 0, -1):
        starts(kv_out(i))
    kx = [(
        rc(k_own, k_all.at[mine, :], kx_s.at[0, 0], kx_r.at[0, 0], x_peer),
        rc(v_ref, v_all.at[mine, :], kx_s.at[1, 0], kx_r.at[1, 0], x_peer),
    )]
    for op in kx[0]:
        op.start()

    def pieces(zz, s_sem, r_sem, i, dev):
        return (
            rc(g_own.at[:, w_cols(zz)], g_all.at[w_rows(sp), :], s_sem.at[0, i], r_sem.at[0, i], dev),
            rc(u_own.at[:, w_cols(zz)], u_all.at[w_rows(sp), :], s_sem.at[1, i], r_sem.at[1, i], dev),
            rc(d_own.at[w_cols(zz), :], d_all.at[sp], s_sem.at[2, i], r_sem.at[2, i], dev),
        )

    for op in loads:
        op.wait()
    wz = []
    for d in range(1, nz):
        wz.append(pieces(up(d), wz_s, wz_r, d, at_z(up(d))))
        for op in wz[-1]:
            op.start()

    for h in range(heads):
        q_s[h] = prepare(q_ref[:, h * hd:(h + 1) * hd], qg_ref[...])
    g_all[w_rows(sp), :] = g_own[:, w_cols(z)]
    u_all[w_rows(sp), :] = u_own[:, w_cols(z)]
    d_all[sp] = d_own[w_cols(z), :]

    for i in range(1, nz):
        t = near(i)
        for op in kv_in(i):
            op.wait_recv()
        theirs = tok_rows(t * NX + x)
        kx.append((
            rc(k_all.at[theirs, :], k_all.at[theirs, :], kx_s.at[0, i], kx_r.at[0, i], x_peer),
            rc(v_all.at[theirs, :], v_all.at[theirs, :], kx_s.at[1, i], kx_r.at[1, i], x_peer),
        ))
        starts(kx[-1])
    wx = [pieces(z, wx_s, wx_r, 0, x_peer)]
    for op in wx[0]:
        op.start()
    for pair in kx:
        for op in pair:
            op.wait_recv()

    scale = hd ** (-0.5)
    for h in range(heads):
        scores = lax.dot_general(
            q_s[h], k_all[...], (((1,), (1,)), ((), ())), preferred_element_type=f32
        )
        top = jnp.max(scores, axis=-1, keepdims=True)
        expo = jnp.exp((scores - top) * scale)
        total = jnp.sum(expo, axis=-1, keepdims=True)
        summed = jnp.dot(expo.astype(bf16), v_all[...], preferred_element_type=f32)
        att_s[:, h * hd:(h + 1) * hd] = (summed / total).astype(bf16)

    step = wide // 4
    for i in range(4):
        cols = slice(i * step, (i + 1) * step)
        prod = jnp.dot(att_s[...], ow_ref[:, cols], preferred_element_type=f32)
        proj[:, :, cols] = prod.astype(bf16).reshape(ntp, rows, step)
    pj = []
    for e in range(1, ntp):
        to = lax.rem(tp + e, ntp)
        pj.append(rc(proj.at[to], proj_in.at[e - 1], pj_s.at[e], pj_r.at[e], (sp, to)))
        pj[-1].start()

    def forward_weights(d):
        for op in wz[d - 1]:
            op.wait_recv()
        s = down(d) * NX + x
        wx.append((
            rc(g_all.at[w_rows(s), :], g_all.at[w_rows(s), :], wx_s.at[0, d], wx_r.at[0, d], x_peer),
            rc(u_all.at[w_rows(s), :], u_all.at[w_rows(s), :], wx_s.at[1, d], wx_r.at[1, d], x_peer),
            rc(d_all.at[s], d_all.at[s], wx_s.at[2, d], wx_r.at[2, d], x_peer),
        ))
        for op in wx[-1]:
            op.start()

    forward_weights(1)
    for op in pj:
        op.wait_recv()
    projected = proj[tp].astype(f32)
    for e in range(1, ntp):
        projected = projected + proj_in[e - 1].astype(f32)
    mixed = (res_ref[...].astype(f32) + projected).astype(bf16)
    mixed_s[...] = mixed
    mixed_f = mixed.astype(f32)
    normed = (
        mixed_f * lax.rsqrt(jnp.mean(mixed_f * mixed_f, axis=-1, keepdims=True) + EPS) * ng_ref[...]
    ).astype(bf16)
    own = z * ntp + tp
    normed_all[own] = normed

    mine_blk = normed_all.at[own]

    def row_out(w, way):
        return rc(mine_blk, mine_blk, nz_s.at[w], nz_r.at[z], line_dev(way))

    def row_in(t, i, dev):
        blk = normed_all.at[t * ntp + tp]
        return rc(blk, blk, af_s.at[i], nz_r.at[t], dev)

    def y_copy(t):
        blk = normed_all.at[t * ntp + tp]
        return rc(blk, blk, ny_s.at[t], ny_r.at[t], y_peer)

    def c_copy(t):
        blk = normed_all.at[t * ntp + tp]
        return rc(blk, blk, nc_s.at[t], nc_r.at[t], c_peer)

    def f_copy(t):
        blk = normed_all.at[t * ntp + (1 - y) * NC + c]
        return rc(blk, blk, nf_s.at[t], nf_r.at[t], c_peer)

    def pass_on(t):
        y_copy(t).start()
        c_copy(t).start()

    def pass_over(t):
        y_copy(t).wait_recv()
        f_copy(t).start()

    for w, (way, ok) in enumerate(ways):
        pl.when(ok)(row_out(w, way).start)
    pass_on(z)
    forward_weights(2)
    pass_over(z)
    forward_weights(3)
    for i in range(1, nz):
        t = near(i)
        dev, inside = onward(t)
        op = row_in(t, i, dev)
        op.wait_recv()
        pl.when(inside)(op.start)
        pass_on(t)
        if i > 1:
            pass_over(near(i - 1))
    for ops in wx:
        for op in ops:
            op.wait_recv()

    def core_ops(t, j):
        b = t * ntp + j * NC + (1 - c)
        return rc(part.at[b], core_in.at[t, j], c_s.at[t, j], c_r.at[t, j], c_peer)

    def y_op(t):
        return rc(y_out.at[t], y_in.at[t], y_s.at[t], y_r.at[t], y_peer)

    def y_stage(t):
        for j in range(2):
            core_ops(t, j).wait_recv()
        b = t * ntp + (1 - y) * NC + c
        y_out[t] = (part[b].astype(f32) + core_in[t, 1 - y].astype(f32)).astype(bf16)
        y_op(t).start()

    cols_each = d_all.shape[2]

    def tile(i, carry):
        t = near(jnp.where(i == 1, 2, jnp.where(i == 2, 1, i)))

        @pl.when(i == nz - 2)
        def _():
            pass_over(near(nz - 1))

        c_copy(t).wait_recv()
        f_copy(t).wait_recv()
        x_t = normed_all[pl.ds(t * ntp, ntp)].reshape(ntp * rows, wide)
        gate = jnp.dot(x_t, g_all[...], preferred_element_type=f32)
        up_val = jnp.dot(x_t, u_all[...], preferred_element_type=f32)
        hidden = (gate / (1.0 + jnp.exp(-gate)) * up_val).astype(bf16)
        for s in range(d_all.shape[0]):
            r = jnp.dot(hidden, d_all[s], preferred_element_type=f32).astype(bf16)
            part[pl.ds(t * ntp, ntp), :, s * cols_each:(s + 1) * cols_each] = r.reshape(ntp, rows, cols_each)
        for j in range(2):
            core_ops(t, j).start()

        @pl.when(i == 2)
        def _():
            y_stage(near(2))

        return carry

    lax.fori_loop(0, nz, tile, 0)

    y_stage(near(3))
    y_stage(near(1))
    y_stage(z)

    def summed_tile(t):
        return part[t * ntp + tp].astype(f32) + core_in[t, y].astype(f32) + y_in[t].astype(f32)

    def z_op(i):
        return rc(z_out.at[i], z_in.at[z], z_s.at[i], z_r.at[z], at_z(near(i)))

    for i in (2, 3, 1):
        t = near(i)
        y_op(t).wait_recv()
        z_out[i] = summed_tile(t).astype(bf16)
        z_op(i).start()
    y_op(z).wait_recv()
    fed = summed_tile(z)
    for i in (2, 3, 1):
        t = near(i)
        rc(z_out.at[i], z_in.at[t], z_s.at[i], z_r.at[t], at_z(t)).wait_recv()
        fed = fed + z_in[t].astype(f32)
    out_ref[...] = (mixed_s[...].astype(f32) + 0.5 * fed).astype(bf16)

    for ops in kx + wz + wx:
        sent(ops)
    sent(pj)
    for w, (way, ok) in enumerate(ways):
        pl.when(ok)(row_out(w, way).wait_send)
    for i in range(nz):
        t = near(i)
        sent((y_copy(t), c_copy(t), f_copy(t), core_ops(t, 0), core_ops(t, 1), y_op(t)))
        if i:
            dev, inside = onward(t)
            pl.when(inside)(row_in(t, i, dev).wait_send)
            sent(kv_out(i))
            z_op(i).wait_send()


def ring_device(
    nsp,
    residual_in, queries, keys_raw, values_raw, query_gain, key_gain, out_weight, norm_gain,
    gate_weight, up_weight, down_weight,
):
    bf16 = jnp.bfloat16
    nz = nsp // NX
    tok = queries.shape[0]
    hd = query_gain.shape[0]
    heads = queries.shape[1] // hd
    rows, wide = residual_in.shape
    drows, units = gate_weight.shape
    ntp = tok // rows
    unit = -(-units // (nz * LANES)) * LANES
    half = hd // 2
    positions = lax.axis_index("sp") * tok + jnp.arange(tok, dtype=jnp.int32)
    freqs = THETA ** (-jnp.arange(0, half, 2, dtype=jnp.float32) / half)
    row_ang = (positions // GRID_W).astype(jnp.float32)[:, None] * freqs
    col_ang = (positions % GRID_W).astype(jnp.float32)[:, None] * freqs
    angles = jnp.concatenate([row_ang, row_ang, col_ang, col_ang], axis=-1)
    sign = jnp.where(jnp.arange(hd) % half < half // 2, -1.0, 1.0)
    cosine, sine = jnp.cos(angles), jnp.sin(angles) * sign
    dma = pltpu.SemaphoreType.DMA
    vm = pltpu.VMEM
    blk = (rows, wide)
    scratch = [
        vm((drows, nz * unit), bf16), vm((drows, nz * unit), bf16), vm((nz * unit, down_weight.shape[1]), bf16),
        vm((tok, hd), bf16), vm((nsp * tok, hd), bf16), vm((nsp * tok, hd), bf16),
        vm((nsp * drows, unit), bf16), vm((nsp * drows, unit), bf16), vm((nsp, unit, down_weight.shape[1]), bf16),
        vm((heads, tok, hd), bf16), vm((tok, heads * hd), bf16),
        vm((ntp,) + blk, bf16), vm((ntp - 1,) + blk, bf16), vm((nz * ntp,) + blk, bf16),
        vm((nz * ntp,) + blk, bf16), vm((nz, 2) + blk, bf16), vm((nz,) + blk, bf16), vm((nz,) + blk, bf16),
        vm((nz,) + blk, bf16), vm((nz,) + blk, bf16), vm(blk, bf16),
        dma((2, nz)), dma((2, nz)), dma((2, nz)), dma((2, nz)),
        dma((3, nz)), dma((3, nz)), dma((3, nz)), dma((3, nz)),
        dma((ntp,)), dma((ntp,)),
    ] + [dma((nz,)) for _ in range(8)] + [
        dma((nz, 2)), dma((nz, 2)), dma((nz,)), dma((nz,)), dma((nz,)), dma((nz,)),
        dma((nz,)), dma((3,)),
    ]
    return pl.pallas_call(
        functools.partial(ring_kernel, nz),
        out_shape=jax.ShapeDtypeStruct(blk, bf16),
        in_specs=[pl.BlockSpec(memory_space=pltpu.VMEM)] * 10 + [pl.BlockSpec(memory_space=pl.ANY)] * 3,
        out_specs=pl.BlockSpec(memory_space=pltpu.VMEM),
        scratch_shapes=scratch,
        compiler_params=pltpu.CompilerParams(
            collective_id=0, has_side_effects=True, vmem_limit_bytes=60 * 1024 * 1024
        ),
    )(
        residual_in, queries, keys_raw, values_raw, cosine, sine, query_gain[None], key_gain[None],
        out_weight, norm_gain[None], gate_weight, up_weight, down_weight,
    )


def solution(mesh):
    nsp, ntp = mesh.shape["sp"], mesh.shape["tp"]

    def per_device(*arrays):
        residual_in, queries, keys_raw = arrays[:3]
        hd = arrays[4].shape[0]
        small = (
            nsp == 8 and ntp == 2 * NC and keys_raw.shape[1] == hd
            and queries.shape[0] == ntp * residual_in.shape[0]
            and arrays[8].shape[0] % LANES == 0 and queries.shape[0] <= 256
        )
        if small:
            return ring_device(nsp, *arrays)
        return plain_device(*arrays)

    placed = (
        P(("sp", "tp"), None),
        P("sp", "tp"),
        P("sp", "tp"),
        P("sp", "tp"),
        P(),
        P(),
        P("tp", None),
        P(),
        P("sp", "tp"),
        P("sp", "tp"),
        P("tp", "sp"),
    )
    return jax.shard_map(
        per_device, mesh=mesh, in_specs=placed, out_specs=P(("sp", "tp"), None), check_vma=False
    )
```
